128 devices in a mesh: sp: 16 (over z, x), tp: 8 (over y, core).
Axes of the slice: x: 4, y: 4, z: 4, core: 2. Of those that a mesh axis runs over, the one named last changes fastest.
Arguments:
- prompt: bfloat16 [4, 8192, 4096], P(None, 'sp'), may hold values from -6 to 6
- key_weight: bfloat16 [4096, 1024], P(None, 'tp'), may hold values from -0.09375 to 0.09375
- value_weight: bfloat16 [4096, 2048], P(None, 'tp'), may hold values from -0.09375 to 0.09375
- input_gate_weight: bfloat16 [4096, 16], P(None, 'tp'), may hold values from -0.09375 to 0.09375
- forget_gate_weight: bfloat16 [4096, 16], P(None, 'tp'), may hold values from -0.09375 to 0.09375
- forget_bias: float32 [16], P('tp'), may hold values from 3 to 11
- key_taps: bfloat16 [3, 1024], P(None, 'tp'), may hold values from -3 to 3
- extra_decay: float32 [4, 8192, 16], P(None, 'sp', 'tp'), may hold values from -1.5 to 0
- new_query: bfloat16 [4, 16, 64], P(None, 'tp'), may hold values from -6 to 6
- new_key: bfloat16 [4, 16, 64], P(None, 'tp'), may hold values from -6 to 6
- new_value: bfloat16 [4, 16, 128], P(None, 'tp', 'sp'), may hold values from -6 to 6
- new_input_gate: float32 [4, 16], P(None, 'tp'), may hold values from 2 to 7
- new_forget_gate: float32 [4, 16], P(None, 'tp'), may hold values from -2 to 4
- out_weight: bfloat16 [16, 128, 4096], P('tp', 'sp'), may hold values from -0.125 to 0.125
Outputs:
- cache_memory: bfloat16 [4, 16, 64, 128], P(None, 'tp', None, 'sp')
- cache_norm: bfloat16 [4, 16, 64], P(None, 'tp', 'sp')
- cache_peak: float32 [4, 16], P(None, 'tp')
- read_out: bfloat16 [4, 4096], P(None, ('sp', 'tp'))
The draws below stay inside these ranges and needn't reach their ends.
All inputs are finite; a program needn't handle non-finite values.
Results may differ from the reference program's by a relative error of at most 0.012.
The reference program's roundings to bfloat16 on the way count: a program that leaves them out, or rounds other values in their place, can miss the bound.
Values may be sent and summed in bfloat16 or wider, within the bound.
A program may use at most 64 MiB of HBM per device.

```python
import math
import jax
import jax.numpy as jnp
from jax import lax

D = 4096
HEAD_TOTAL = 16
KEY_DIM = 64
VALUE_DIM = 128
TAPS = 3
PROMPT_COUNT = 4
SEG = 512
PROMPT_LENGTH = 8192


def draw_forget_bias(key, part):
    first_key, second_key, third_key = jax.random.split(key, 3)
    chooser = jax.random.uniform(first_key, (HEAD_TOTAL,), jnp.float32)
    share = 0.5
    quick_bias = jax.random.uniform(second_key, (HEAD_TOTAL,), jnp.float32, 3.0, 4.2)
    steady_bias = jnp.log(jnp.float32(PROMPT_LENGTH)) + jax.random.uniform(third_key, (HEAD_TOTAL,), jnp.float32, 1.5, 3.0)
    steady_bias = jnp.minimum(steady_bias, 11.0)
    return jnp.where(chooser < share, quick_bias, steady_bias)


def draw_extra_decay(key, part):
    key_seg, key_location, key_depth = jax.random.split(key, 3)
    blocks = PROMPT_LENGTH // SEG
    seg_log = jax.random.uniform(key_seg, (PROMPT_COUNT, blocks, HEAD_TOTAL), jnp.float32, math.log(0.005), math.log(0.05))
    stable_offset = jnp.repeat(-jnp.exp(seg_log) / SEG, SEG, axis=1)
    spike_location = jax.random.randint(key_location, (PROMPT_COUNT, 2, HEAD_TOTAL), 0, PROMPT_LENGTH)
    depth_limit = jax.random.uniform(key_depth, (PROMPT_COUNT, 2, HEAD_TOTAL), jnp.float32, 0.22, 0.7)
    token_position = jnp.arange(PROMPT_LENGTH)
    hit_values = token_position[None, :, None, None] == spike_location[:, None, :, :]
    spike_values = jnp.sum(jnp.where(hit_values, -depth_limit[:, None, :, :], 0.0), axis=2)
    return stable_offset + spike_values


def levels(key, dims, pieces, smallest, top_value):
    gain = 1.0
    for dim, parts in pieces:
        draws = jax.random.uniform(jax.random.fold_in(jax.random.fold_in(key, 6), dim), (parts,), jnp.float32, smallest / len(pieces), top_value / len(pieces))
        gain = gain * jnp.repeat(jnp.exp(draws), dims[dim] // parts).reshape((-1,) + (1,) * (len(dims) - 1 - dim))
    return gain


def scatter_about(own_key, shape, width, limit, shards=(), held_as=jnp.bfloat16):
    level = levels(own_key, shape, shards, -0.22, 0.18) if shards else 1.0
    drawn = jax.random.normal(own_key, shape, jnp.float32) * width * level
    return jnp.minimum(jnp.maximum(drawn, -limit), limit).astype(held_as)


def setup_inputs(seed: int = 0) -> dict:
    seeds = jax.random.split(jax.random.key(seed), 15)
    prompt = scatter_about(seeds[0], (PROMPT_COUNT, PROMPT_LENGTH, D), 1.0, 6.0, ((1, 16),))
    key_weight = scatter_about(seeds[1], (D, HEAD_TOTAL * KEY_DIM), D ** -0.5, 0.09375, ((1, 8),))
    value_weight = scatter_about(seeds[2], (D, HEAD_TOTAL * VALUE_DIM), D ** -0.5, 0.09375, ((1, 8),))
    input_gate_weight = scatter_about(seeds[3], (D, HEAD_TOTAL), D ** -0.5, 0.09375, ((1, 8),))
    forget_gate_weight = scatter_about(seeds[4], (D, HEAD_TOTAL), D ** -0.5, 0.09375, ((1, 8),))
    forget_bias = draw_forget_bias(jax.random.fold_in(seeds[14], 71), 0)
    key_taps = scatter_about(seeds[6], (TAPS, HEAD_TOTAL * KEY_DIM), 0.577, 3.0, ((1, 8),))
    extra_decay = draw_extra_decay(jax.random.fold_in(seeds[14], 71), 0)
    new_query = scatter_about(seeds[8], (PROMPT_COUNT, HEAD_TOTAL, KEY_DIM), 1.0, 6.0, ((1, 8),))
    new_key = scatter_about(seeds[9], (PROMPT_COUNT, HEAD_TOTAL, KEY_DIM), 1.0, 6.0, ((1, 8),))
    new_value = scatter_about(seeds[10], (PROMPT_COUNT, HEAD_TOTAL, VALUE_DIM), 1.0, 6.0, ((1, 8), (2, 16)))
    new_input_gate = jnp.clip(2.0 + 5.0 * jax.random.uniform(seeds[11], (PROMPT_COUNT, HEAD_TOTAL), jnp.float32) ** levels(seeds[11], (PROMPT_COUNT, HEAD_TOTAL), ((1, 8),), -0.2, 0.2), 2.0, 7.0)
    new_forget_gate = jnp.clip(-2.0 + 6.0 * jax.random.uniform(seeds[12], (PROMPT_COUNT, HEAD_TOTAL), jnp.float32) ** levels(seeds[12], (PROMPT_COUNT, HEAD_TOTAL), ((1, 8),), -0.2, 0.2), -2.0, 4.0)
    out_weight = scatter_about(seeds[13], (HEAD_TOTAL, VALUE_DIM, D), (HEAD_TOTAL * VALUE_DIM) ** -0.5, 0.125, ((0, 8), (1, 16)))
    return dict(prompt=prompt, key_weight=key_weight, value_weight=value_weight, input_gate_weight=input_gate_weight, forget_gate_weight=forget_gate_weight, forget_bias=forget_bias, key_taps=key_taps, extra_decay=extra_decay, new_query=new_query, new_key=new_key, new_value=new_value, new_input_gate=new_input_gate, new_forget_gate=new_forget_gate, out_weight=out_weight)


def widen(rounded):
    return lax.optimization_barrier(rounded).astype(jnp.float32)


def key_conv(key_raw, key_taps):
    padded = jnp.pad(key_raw, ((1, 1), (0, 0)))
    tap_f32 = key_taps.astype(jnp.float32)
    mixed = tap_f32[0] * padded[:-2] + tap_f32[1] * padded[1:-1] + tap_f32[2] * padded[2:]
    return (jax.nn.silu(mixed) * KEY_DIM ** -0.5).astype(jnp.bfloat16)


def reference(prompt, key_weight, value_weight, input_gate_weight, forget_gate_weight, forget_bias,
              key_taps, extra_decay, new_query, new_key, new_value, new_input_gate, new_forget_gate,
              out_weight):
    def prompt_state(inputs):
        seq_rows, seq_extra = inputs
        key_raw = jnp.dot(seq_rows, key_weight, preferred_element_type=jnp.float32).astype(jnp.bfloat16)
        values = jnp.dot(seq_rows, value_weight, preferred_element_type=jnp.float32).astype(jnp.bfloat16)
        input_pre = widen(jnp.dot(seq_rows, input_gate_weight, preferred_element_type=jnp.float32).astype(jnp.bfloat16))
        forget_pre = widen(jnp.dot(seq_rows, forget_gate_weight, preferred_element_type=jnp.float32).astype(jnp.bfloat16))
        key_rows = key_conv(key_raw, key_taps)
        log_forget = jax.nn.log_sigmoid(forget_pre + forget_bias) + seq_extra
        suffix = jnp.sum(log_forget, axis=0, keepdims=True) - jnp.cumsum(log_forget, axis=0)
        gate_log = input_pre + suffix
        peak_log = jnp.max(gate_log, axis=0)
        scale = jnp.exp(gate_log - peak_log[None])
        key_quartet = key_rows.reshape(PROMPT_LENGTH, HEAD_TOTAL, KEY_DIM).astype(jnp.float32)
        value_four = values.reshape(PROMPT_LENGTH, HEAD_TOTAL, VALUE_DIM)
        weighted_rows = (value_four * scale[:, :, None]).astype(jnp.bfloat16)
        memory_matrix = jnp.einsum('xje,xjb->jeb', key_quartet, weighted_rows.astype(jnp.float32))
        normer = jnp.einsum('lh,lhk->hk', scale, key_quartet, precision=lax.Precision.HIGHEST)
        return memory_matrix, normer, peak_log

    memory_matrix, normer, peak_log = lax.map(prompt_state, (prompt, extra_decay))
    forget_new = jax.nn.log_sigmoid(new_forget_gate)
    new_peak = jnp.maximum(forget_new + peak_log, new_input_gate)
    old_scale = jnp.exp(forget_new + peak_log - new_peak)
    new_scale = jnp.exp(new_input_gate - new_peak)
    key_new = new_key.astype(jnp.float32)
    value_new = new_value.astype(jnp.float32)
    memory_next = (old_scale[:, :, None, None] * memory_matrix
                   + new_scale[:, :, None, None] * key_new[:, :, :, None] * value_new[:, :, None, :])
    normer_next = old_scale[:, :, None] * normer + new_scale[:, :, None] * key_new
    query = new_query.astype(jnp.float32)
    numer = jnp.sum(query[:, :, :, None] * memory_next, axis=2)
    denom = jnp.sum(query * normer_next, axis=-1)
    read = (numer / jnp.maximum(jnp.abs(denom), 1.0)[:, :, None]).astype(jnp.bfloat16)
    read_out = jnp.dot(read.reshape(PROMPT_COUNT, HEAD_TOTAL * VALUE_DIM), out_weight.reshape(HEAD_TOTAL * VALUE_DIM, D),
                       preferred_element_type=jnp.float32).astype(jnp.bfloat16)
    return memory_matrix.astype(jnp.bfloat16), normer.astype(jnp.bfloat16), peak_log, read_out
```

```python
import jax
import jax.numpy as jnp
from jax import lax
from jax.experimental import pallas as pl
from jax.experimental.pallas import tpu as pltpu
from jax.sharding import PartitionSpec as P

MESH_ID = pl.DeviceIdType.MESH
F32 = jnp.float32
BF16 = jnp.bfloat16
NT = (((1,), (1,)), ((), ()))
KEY0 = 16
VAL0 = 144
CHUNKS = 4


def log_sigmoid(x):
    return jnp.minimum(x, 0.0) - jnp.log1p(jnp.exp(-jnp.abs(x)))


def three_parts(x):
    high = x.astype(BF16)
    rest = x - high.astype(F32)
    middle = rest.astype(BF16)
    low = (rest - middle.astype(F32)).astype(BF16)
    return high, middle, low


def kernel(
    prompt, key_w, value_w, in_w, fg_w, fg_bias, taps, extra, query, new_key, new_value,
    new_in, new_fg, out_w,
    mem_out, norm_out, peak_out, read_out,
    p_buf, wk_buf, wv_buf, wt_buf, hp_buf, r_buf, par_buf, mem_buf, e_buf,
    h_send, h_recv, e_recv, m_recv, ow_recv, part_buf, part_recv,
    w_sem, p_sem, hp_sem, ow_local, h_ssem, h_rsem, e_ssem, e_rsem, m_ssem, m_rsem,
    ow_ssem, ow_rsem, o_ssem, o_rsem,
):
    seqs, length, width = p_buf.shape
    sp_n, tp_n = lax.axis_size("sp"), lax.axis_size("tp")
    sp, tp = lax.axis_index("sp"), lax.axis_index("tp")
    step = width // CHUNKS

    barrier = pltpu.get_barrier_semaphore()

    def sp_peer(d):
        return lax.rem(sp + d, sp_n)

    def tp_peer(d):
        return lax.rem(tp + d, tp_n)

    @pl.loop(1, sp_n)
    def _(d):
        pl.semaphore_signal(barrier, inc=1, device_id=(sp_peer(d), tp), device_id_type=MESH_ID)

    @pl.loop(1, tp_n)
    def _(d):
        pl.semaphore_signal(barrier, inc=1, device_id=(sp, tp_peer(d)), device_id_type=MESH_ID)

    hp_copies = []
    for s in range(seqs):
        for side, row in ((0, 0), (1, length - 8)):
            g = 2 * s + side
            hp_copies.append(
                pltpu.make_async_copy(
                    prompt.at[s, pl.ds(row, 8), :], hp_buf.at[pl.ds(8 * g, 8), :], hp_sem.at[g]
                )
            )
    w_copies, p_copies = [], []
    for c in range(CHUNKS):
        rows = pl.ds(c * step, step)
        w_copies.append(
            (
                pltpu.make_async_copy(key_w.at[rows, :], wk_buf.at[rows, :], w_sem.at[0, c]),
                pltpu.make_async_copy(value_w.at[rows, :], wv_buf.at[rows, :], w_sem.at[1, c]),
            )
        )
        p_copies.append(
            pltpu.make_async_copy(prompt.at[0, :, rows], p_buf.at[0, :, rows], p_sem.at[0, c])
        )
    for c in range(CHUNKS):
        for copy in w_copies[c]:
            copy.start()
        p_copies[c].start()
        if c == 0:
            for copy in hp_copies:
                copy.start()
    s_copies = [None]
    for s in range(1, seqs):
        group = []
        for c in range(CHUNKS):
            rows = pl.ds(c * (length // CHUNKS), length // CHUNKS)
            group.append(
                pltpu.make_async_copy(prompt.at[s, rows, :], p_buf.at[s, rows, :], p_sem.at[s, c])
            )
        for copy in group:
            copy.start()
        s_copies.append(group)

    lane = lax.broadcasted_iota(jnp.int32, (1, 128), 1)
    first_head = lane < 64

    def halves(left, right):
        return jnp.where(first_head, left, right)

    for s in range(seqs):
        rows = pl.ds(s, 1)
        par_buf[0, rows, :] = jnp.concatenate(
            [query[s, 0:1, :].astype(F32), query[s, 1:2, :].astype(F32)], axis=1
        )
        par_buf[1, rows, :] = jnp.concatenate(
            [new_key[s, 0:1, :].astype(F32), new_key[s, 1:2, :].astype(F32)], axis=1
        )
        par_buf[2, rows, :] = halves(new_in[0:1, s : s + 1], new_in[1:2, s : s + 1])
        par_buf[3, rows, :] = halves(new_fg[0:1, s : s + 1], new_fg[1:2, s : s + 1])
    tap_cols = jnp.transpose(
        jnp.concatenate([taps[...].astype(F32), jnp.zeros((5, 128), F32)], axis=0)
    )
    q_cols = jnp.transpose(
        jnp.concatenate([par_buf[0, 0:4, :], jnp.zeros((4, 128), F32)], axis=0)
    )
    gate_rows = jnp.concatenate(
        [
            in_w[...].astype(F32), jnp.zeros((6, width), F32),
            fg_w[...].astype(F32), jnp.zeros((6, width), F32),
        ],
        axis=0,
    )
    wt_buf[0:KEY0, :] = gate_rows.astype(BF16)

    for c in range(CHUNKS):
        cols = pl.ds(c * step, step)
        for copy in w_copies[c]:
            copy.wait()
        wt_buf[KEY0:VAL0, cols] = jnp.transpose(wk_buf[cols, :])
        wt_buf[VAL0:, cols] = jnp.transpose(wv_buf[cols, :])
        p_copies[c].wait()
        part = lax.dot_general(
            wt_buf[:, cols], p_buf[0, :, cols], NT, preferred_element_type=F32
        )
        if c == 0:
            r_buf[0] = part
        else:
            r_buf[0] = r_buf[0] + part

    for copy in hp_copies:
        copy.wait()
    edge = jnp.dot(hp_buf[...], wk_buf[...], preferred_element_type=F32).astype(BF16).astype(F32)
    zero4 = jnp.zeros((4, 128), F32)
    h_send[0] = jnp.concatenate(
        [edge[16 * s + 15 : 16 * s + 16] for s in range(seqs)] + [zero4], axis=0
    )
    h_send[1] = jnp.concatenate(
        [edge[16 * s : 16 * s + 1] for s in range(seqs)] + [zero4], axis=0
    )

    pl.semaphore_wait(barrier, sp_n - 1 + tp_n - 1)

    cols_of = out_w.shape[2] // sp_n

    def ow_slot(ref):
        return ref.at[sp // 8, :, lax.rem(sp, 8)]

    def ow_cols(j):
        return out_w.at[:, :, pl.ds(pl.multiple_of(j * cols_of, cols_of), cols_of)]

    own_ow = pltpu.make_async_copy(ow_cols(sp), ow_slot(ow_recv), ow_local)
    own_ow.start()

    halo_copies = []
    for side, d in ((0, 1), (1, sp_n - 1)):
        copy = pltpu.make_async_remote_copy(
            src_ref=h_send.at[side],
            dst_ref=h_recv.at[side],
            send_sem=h_ssem.at[side],
            recv_sem=h_rsem.at[side],
            device_id=(sp_peer(d), tp),
            device_id_type=MESH_ID,
        )
        copy.start()
        halo_copies.append(copy)

    @pl.loop(1, sp_n)
    def _(d):
        j = sp_peer(d)
        pltpu.make_async_remote_copy(
            src_ref=ow_cols(j),
            dst_ref=ow_slot(ow_recv),
            send_sem=ow_ssem,
            recv_sem=ow_rsem,
            device_id=(j, tp),
            device_id_type=MESH_ID,
        ).start()

    def edges():
        for copy in halo_copies:
            copy.wait_recv()
        before = jnp.where(sp == 0, 0.0, jnp.transpose(h_recv[0]))
        after = jnp.where(sp == sp_n - 1, 0.0, jnp.transpose(h_recv[1]))
        return before, after

    pos = lax.broadcasted_iota(jnp.int32, (1, length), 1)
    my_rows = pl.multiple_of(8 * sp, 8)

    def slot_rows(s):
        return pl.ds(pl.multiple_of((s * sp_n + sp) * 8, 8), 8)

    def finish(s, before, after):
        buf = s % 2
        in_pre = r_buf[buf, 0:2, :].astype(BF16).astype(F32)
        fg_pre = r_buf[buf, 8:10, :].astype(BF16).astype(F32)
        log_f = log_sigmoid(fg_pre + fg_bias[...]) + extra[s]
        later = jnp.where(pos < length - 1, pltpu.roll(log_f, length - 1, 1), 0.0)
        shift = 1
        while shift < length:
            later = later + jnp.where(
                pos < length - shift, pltpu.roll(later, length - shift, 1), 0.0
            )
            shift *= 2
        total = later[:, 0:1] + log_f[:, 0:1]
        gate = in_pre + later
        top = jnp.max(gate, axis=1, keepdims=True)
        scale = jnp.exp(gate - top)

        key = r_buf[buf, KEY0:VAL0, :].astype(BF16).astype(F32)
        earlier = jnp.where(pos == 0, before[:, s : s + 1], pltpu.roll(key, 1, 1))
        coming = jnp.where(pos == length - 1, after[:, s : s + 1], pltpu.roll(key, length - 1, 1))
        mixed = tap_cols[:, 0:1] * earlier + tap_cols[:, 1:2] * key + tap_cols[:, 2:3] * coming
        key_rows = (mixed * jax.nn.sigmoid(mixed) * 0.125).astype(BF16)
        prod = key_rows.astype(F32) * q_cols[:, s : s + 1]
        along = jnp.concatenate(
            [
                jnp.sum(prod[0:64], axis=0, keepdims=True),
                jnp.sum(prod[64:128], axis=0, keepdims=True),
            ],
            axis=0,
        )
        value = r_buf[buf, VAL0:, :].astype(BF16).astype(F32)
        weighted = jnp.concatenate(
            [
                (value[0:128] * scale[0:1]).astype(BF16),
                (value[128:256] * scale[1:2]).astype(BF16),
            ],
            axis=0,
        )

        def rows_of(x):
            parts = [part.astype(F32) for part in three_parts(x)]
            return jnp.concatenate(parts + [jnp.zeros((10, length), F32)], axis=0).astype(BF16)

        norm_parts = lax.dot_general(rows_of(scale), key_rows, NT, preferred_element_type=F32)
        num_parts = lax.dot_general(rows_of(along), weighted, NT, preferred_element_type=F32)
        outer = lax.dot_general(weighted, key_rows, NT, preferred_element_type=F32)
        mem_buf[pl.ds(128 * s, 128), :] = halves(outer[0:128], outer[128:256])

        def joined(x, h):
            return x[h : h + 1] + x[2 + h : 3 + h] + x[4 + h : 5 + h]

        norm = halves(joined(norm_parts, 0), joined(norm_parts, 1))
        num0 = joined(num_parts, 0)[:, 0:128]
        num1 = joined(num_parts, 1)[:, 128:256]
        num_a = halves(num0, pltpu.roll(num1, 64, 1))
        num_b = halves(pltpu.roll(num0, 64, 1), num1)

        fresh = new_value[s].astype(F32)
        spread = jnp.concatenate([fresh, jnp.zeros((2, 120), F32)], axis=1)
        left = pltpu.roll(spread, 8 * lax.rem(sp, 8), 1)
        fresh_row = halves(left[0:1], pltpu.roll(left[1:2], 64, 1))
        fresh_a = jnp.where(sp < 8, fresh_row, 0.0)
        fresh_b = jnp.where(sp < 8, 0.0, fresh_row)
        tile = jnp.concatenate(
            [
                norm,
                halves(total[0:1], total[1:2]),
                halves(top[0:1], top[1:2]),
                num_a,
                num_b,
                fresh_a,
                fresh_b,
                jnp.zeros((1, 128), F32),
            ],
            axis=0,
        )
        e_buf[pl.ds(8 * s, 8), :] = tile
        e_recv[slot_rows(s), :] = tile
        m_recv[slot_rows(s), :] = mem_buf[pl.ds(128 * s + my_rows, 8), :]

        @pl.loop(1, sp_n)
        def _(d):
            pltpu.make_async_remote_copy(
                src_ref=e_buf.at[pl.ds(8 * s, 8), :],
                dst_ref=e_recv.at[slot_rows(s), :],
                send_sem=e_ssem.at[s],
                recv_sem=e_rsem.at[s],
                device_id=(sp_peer(d), tp),
                device_id_type=MESH_ID,
            ).start()

        @pl.loop(1, sp_n)
        def _(d):
            j = sp_peer(d)
            pltpu.make_async_remote_copy(
                src_ref=mem_buf.at[pl.ds(pl.multiple_of(128 * s + 8 * j, 8), 8), :],
                dst_ref=m_recv.at[slot_rows(s), :],
                send_sem=m_ssem.at[s],
                recv_sem=m_rsem.at[s],
                device_id=(j, tp),
                device_id_type=MESH_ID,
            ).start()

    before = after = None
    for s in range(1, seqs):
        for copy in s_copies[s]:
            copy.wait()
        if s == 1:
            before, after = edges()
        r_buf[s % 2] = lax.dot_general(wt_buf[...], p_buf[s], NT, preferred_element_type=F32)
        finish(s - 1, before, after)
    finish(seqs - 1, before, after)

    def take(ref, sem, count):
        view = ref.at[pl.ds(0, count), :]
        pltpu.make_async_copy(view, view, sem).wait()

    own_ow.wait()

    row16 = lax.broadcasted_iota(jnp.int32, (sp_n, 128), 0)
    reads, factors = [], []
    for s in range(seqs):
        take(e_recv, e_rsem.at[s], 8 * (sp_n - 1))
    for s in range(seqs):

        def rows_at(k):
            return e_recv[pl.ds(s * sp_n * 8 + k, sp_n, stride=8), :]

        later = jnp.where(row16 < sp_n - 1, pltpu.roll(rows_at(1), sp_n - 1, 0), 0.0)
        shift = 1
        while shift < sp_n:
            later = later + jnp.where(
                row16 < sp_n - shift, pltpu.roll(later, sp_n - shift, 0), 0.0
            )
            shift *= 2
        gate = rows_at(2) + later
        peak = jnp.max(gate, axis=0, keepdims=True)
        factor = jnp.exp(gate - peak)
        factors.append(factor)

        def summed(k):
            return jnp.sum(factor * rows_at(k), axis=0, keepdims=True)

        norm, num_a, num_b = summed(0), summed(3), summed(4)
        fresh_a = jnp.sum(rows_at(5), axis=0, keepdims=True)
        fresh_b = jnp.sum(rows_at(6), axis=0, keepdims=True)
        q, k = par_buf[0, s : s + 1, :], par_buf[1, s : s + 1, :]
        gate_in, gate_fg = par_buf[2, s : s + 1, :], par_buf[3, s : s + 1, :]
        kept = log_sigmoid(gate_fg) + peak
        new_peak = jnp.maximum(kept, gate_in)
        old_scale = jnp.exp(kept - new_peak)
        new_scale = jnp.exp(gate_in - new_peak)

        def by_head(x):
            left = jnp.sum(jnp.where(first_head, x, 0.0), axis=1, keepdims=True)
            right = jnp.sum(jnp.where(first_head, 0.0, x), axis=1, keepdims=True)
            return halves(left, right)

        denom = jnp.maximum(jnp.abs(by_head(q * (old_scale * norm + new_scale * k))), 1.0)
        fresh_scale = new_scale * by_head(q * k)
        read_a = (old_scale * num_a + fresh_scale * fresh_a) / denom
        read_b = (old_scale * num_b + fresh_scale * fresh_b) / denom
        reads.append(jnp.concatenate([read_a, read_b], axis=1))
        mine = pltpu.roll(norm, lax.rem(128 - 4 * sp, 128), 1).astype(BF16)
        norm_out[s, 0:1, :] = mine[:, 0:4]
        norm_out[s, 1:2, :] = mine[:, 64:68]
        peak_out[0:1, s : s + 1] = peak[:, 0:1]
        peak_out[1:2, s : s + 1] = peak[:, 64:65]

    ow_words = pltpu.make_async_copy(
        out_w.at[:, :, pl.ds(0, cols_of * (sp_n - 1))],
        out_w.at[:, :, pl.ds(0, cols_of * (sp_n - 1))],
        ow_rsem,
    )
    ow_words.wait()
    read = jnp.concatenate(reads + [jnp.zeros((12, 256), F32)], axis=0).astype(BF16)
    weight = ow_recv[...].reshape(256, cols_of)
    part = jnp.dot(read, weight, preferred_element_type=F32)[0:8]
    part_buf[...] = part
    part_recv[tp] = part

    @pl.loop(1, tp_n)
    def _(d):
        pltpu.make_async_remote_copy(
            src_ref=part_buf,
            dst_ref=part_recv.at[tp],
            send_sem=o_ssem,
            recv_sem=o_rsem,
            device_id=(sp, tp_peer(d)),
            device_id_type=MESH_ID,
        ).start()

    for s in range(seqs):
        take(m_recv, m_rsem.at[s], 8 * (sp_n - 1))
    for s in range(seqs):
        memory = jnp.zeros((8, 128), F32)
        for i in range(sp_n):
            base = (s * sp_n + i) * 8
            memory = memory + factors[s][i : i + 1] * m_recv[base : base + 8, :]
        mem_out[s, 0] = memory[:, 0:64].astype(BF16)
        mem_out[s, 1] = memory[:, 64:128].astype(BF16)

    view = part_recv.at[pl.ds(0, tp_n - 1)]
    pltpu.make_async_copy(view, view, o_rsem).wait()
    whole = part_recv[0]
    for i in range(1, tp_n):
        whole = whole + part_recv[i]
    turned = pltpu.roll(whole, lax.rem(cols_of - 32 * tp, cols_of), 1)
    read_out[...] = turned[0:4, 0:32].astype(BF16)

    for copy in halo_copies:
        copy.wait_send()
    pltpu.make_async_copy(
        out_w.at[:, :, pl.ds(0, cols_of * (sp_n - 1))],
        out_w.at[:, :, pl.ds(0, cols_of * (sp_n - 1))],
        ow_ssem,
    ).wait()
    for s in range(seqs):
        take(e_recv, e_ssem.at[s], 8 * (sp_n - 1))
        take(m_recv, m_ssem.at[s], 8 * (sp_n - 1))
    pltpu.make_async_copy(view, view, o_ssem).wait()


def body(
    prompt, key_weight, value_weight, input_gate_weight, forget_gate_weight, forget_bias,
    key_taps, extra_decay, new_query, new_key, new_value, new_input_gate, new_forget_gate,
    out_weight,
):
    seqs, length, width = prompt.shape
    sp_n = lax.axis_size("sp")
    tp_n = lax.axis_size("tp")
    cols_of = out_weight.shape[2] // sp_n
    any_spec = pl.BlockSpec(memory_space=pl.ANY)
    vmem = pl.BlockSpec(memory_space=pltpu.VMEM)
    dma = pltpu.SemaphoreType.DMA
    memory, norm, peak, read = pl.pallas_call(
        kernel,
        out_shape=(
            jax.ShapeDtypeStruct((seqs, 2, 8, 64), BF16),
            jax.ShapeDtypeStruct((seqs, 2, 4), BF16),
            jax.ShapeDtypeStruct((2, seqs), F32),
            jax.ShapeDtypeStruct((seqs, 32), BF16),
        ),
        in_specs=[any_spec] * 3 + [vmem] * 10 + [any_spec],
        out_specs=(vmem,) * 4,
        scratch_shapes=[
            pltpu.VMEM((seqs, length, width), BF16),
            pltpu.VMEM((width, 128), BF16),
            pltpu.VMEM((width, 256), BF16),
            pltpu.VMEM((400, width), BF16),
            pltpu.VMEM((64, width), BF16),
            pltpu.VMEM((2, 400, length), F32),
            pltpu.VMEM((4, 8, 128), F32),
            pltpu.VMEM((seqs * 128, 128), F32),
            pltpu.VMEM((seqs * 8, 128), F32),
            pltpu.VMEM((2, 8, 128), F32),
            pltpu.VMEM((2, 8, 128), F32),
            pltpu.VMEM((seqs * sp_n * 8, 128), F32),
            pltpu.VMEM((seqs * sp_n * 8, 128), F32),
            pltpu.VMEM((2, 2, 8, 8, cols_of), BF16),
            pltpu.VMEM((8, cols_of), F32),
            pltpu.VMEM((tp_n, 8, cols_of), F32),
            dma((2, CHUNKS)),
            dma((seqs, CHUNKS)),
            dma((2 * seqs,)),
            dma,
            dma((2,)),
            dma((2,)),
            dma((seqs,)),
            dma((seqs,)),
            dma((seqs,)),
            dma((seqs,)),
            dma,
            dma,
            dma,
            dma,
        ],
        compiler_params=pltpu.CompilerParams(
            collective_id=0, has_side_effects=True, vmem_limit_bytes=60 * 1024 * 1024
        ),
        name="prompt_state",
    )(
        prompt,
        key_weight,
        value_weight,
        input_gate_weight.T,
        forget_gate_weight.T,
        forget_bias.reshape(2, 1),
        key_taps,
        jnp.transpose(extra_decay, (0, 2, 1)),
        new_query,
        new_key,
        new_value,
        new_input_gate.T,
        new_forget_gate.T,
        out_weight,
    )
    return jnp.transpose(memory, (0, 1, 3, 2)), norm, peak.T, read


def solution(mesh):
    in_specs = (
        P(None, "sp", None),
        P(None, "tp"),
        P(None, "tp"),
        P(None, "tp"),
        P(None, "tp"),
        P("tp"),
        P(None, "tp"),
        P(None, "sp", "tp"),
        P(None, "tp", None),
        P(None, "tp", None),
        P(None, "tp", "sp"),
        P(None, "tp"),
        P(None, "tp"),
        P("tp", "sp", None),
    )
    out_specs = (
        P(None, "tp", None, "sp"),
        P(None, "tp", "sp"),
        P(None, "tp"),
        P(None, ("sp", "tp")),
    )
    return jax.shard_map(body, mesh=mesh, in_specs=in_specs, out_specs=out_specs, check_vma=False)
```

```python
import jax
import jax.numpy as jnp
from jax import lax
from jax.experimental import pallas as pl
from jax.experimental.pallas import tpu as pltpu
from jax.sharding import PartitionSpec as P

MESH_ID = pl.DeviceIdType.MESH
F32 = jnp.float32
BF16 = jnp.bfloat16
NT = (((1,), (1,)), ((), ()))
KEY0 = 16
VAL0 = 144
CHUNKS = 4


def log_sigmoid(x):
    return jnp.minimum(x, 0.0) - jnp.log1p(jnp.exp(-jnp.abs(x)))


def three_parts(x):
    high = x.astype(BF16)
    rest = x - high.astype(F32)
    middle = rest.astype(BF16)
    low = (rest - middle.astype(F32)).astype(BF16)
    return high, middle, low


def kernel(
    prompt, key_w, value_w, in_w, fg_w, fg_bias, taps, extra, query, new_key, new_value,
    new_in, new_fg, out_w,
    packed,
    p_buf, wk_buf, wv_buf, wt_buf, hp_buf, r_buf, tri_buf, par_buf, mem_buf, e_buf,
    h_send, h_recv, e_recv, m_recv, ow_recv, part_buf, part_recv,
    in_v, fg_v, bias_v, taps_v, extra_v, query_v, key_v, value_v, nin_v, nfg_v,
    w_sem, p_sem, hp_sem, small_sem, ow_local, h_ssem, h_rsem, e_ssem, e_rsem, m_ssem, m_rsem,
    ow_ssem, ow_rsem, o_ssem, o_rsem,
):
    seqs, length, width = p_buf.shape
    sp_n, tp_n = lax.axis_size("sp"), lax.axis_size("tp")
    sp, tp = lax.axis_index("sp"), lax.axis_index("tp")
    step = width // CHUNKS

    barrier = pltpu.get_barrier_semaphore()

    def sp_peer(d):
        return lax.rem(sp + d, sp_n)

    def tp_peer(d):
        return lax.rem(tp + d, tp_n)

    small_pairs = (
        (in_w, in_v), (fg_w, fg_v), (fg_bias, bias_v), (taps, taps_v), (extra, extra_v),
        (query, query_v), (new_key, key_v), (new_value, value_v), (new_in, nin_v),
        (new_fg, nfg_v),
    )
    small_copies = [
        pltpu.make_async_copy(src, dst, small_sem.at[i])
        for i, (src, dst) in enumerate(small_pairs)
    ]
    hp_copies = []
    for s in range(seqs):
        for side, row in ((0, 0), (1, length - 8)):
            g = 2 * s + side
            hp_copies.append(
                pltpu.make_async_copy(
                    prompt.at[s, pl.ds(row, 8), :], hp_buf.at[pl.ds(8 * g, 8), :], hp_sem.at[g]
                )
            )
    w_copies, p_copies = [], []
    for c in range(CHUNKS):
        rows = pl.ds(c * step, step)
        w_copies.append(
            (
                pltpu.make_async_copy(key_w.at[rows, :], wk_buf.at[rows, :], w_sem.at[0, c]),
                pltpu.make_async_copy(value_w.at[rows, :], wv_buf.at[rows, :], w_sem.at[1, c]),
            )
        )
        p_copies.append(
            pltpu.make_async_copy(prompt.at[0, :, rows], p_buf.at[0, :, rows], p_sem.at[0, c])
        )
    s_copies = [p_copies]
    for s in range(1, seqs):
        group = []
        for c in range(CHUNKS):
            rows = pl.ds(c * (length // CHUNKS), length // CHUNKS)
            group.append(
                pltpu.make_async_copy(prompt.at[s, rows, :], p_buf.at[s, rows, :], p_sem.at[s, c])
            )
        s_copies.append(group)

    def start(copies):
        for copy in copies:
            copy.start()

    def finished(copies):
        for copy in copies:
            copy.wait()

    start(small_copies[:2])
    start(w_copies[0])
    start(p_copies[0:1])
    start(small_copies[2:])
    start(w_copies[1])
    start(p_copies[1:2])
    start(hp_copies)

    @pl.loop(1, sp_n)
    def _(d):
        pl.semaphore_signal(barrier, inc=1, device_id=(sp_peer(d), tp), device_id_type=MESH_ID)

    @pl.loop(1, tp_n)
    def _(d):
        pl.semaphore_signal(barrier, inc=1, device_id=(sp, tp_peer(d)), device_id_type=MESH_ID)

    tri_buf[...] = (
        lax.broadcasted_iota(jnp.int32, (length, length), 0)
        > lax.broadcasted_iota(jnp.int32, (length, length), 1)
    ).astype(F32).astype(BF16)

    lane = lax.broadcasted_iota(jnp.int32, (1, 128), 1)
    first_head = lane < 64

    def halves(left, right):
        return jnp.where(first_head, left, right)

    def chunk_of(c):
        return pl.ds(c * step, step)

    def turn(c):
        cols = chunk_of(c)
        wt_buf[KEY0:VAL0, cols] = jnp.transpose(wk_buf[cols, :])
        wt_buf[VAL0:, cols] = jnp.transpose(wv_buf[cols, :])

    def chunk_dot(c):
        cols = chunk_of(c)
        part = lax.dot_general(
            wt_buf[:, cols], p_buf[0, :, cols], NT, preferred_element_type=F32
        )
        if c == 0:
            r_buf[0] = part
        else:
            r_buf[0] = r_buf[0] + part

    finished(small_copies[:2])
    gate_rows = jnp.concatenate(
        [
            in_v[...].astype(F32), jnp.zeros((6, width), F32),
            fg_v[...].astype(F32), jnp.zeros((6, width), F32),
        ],
        axis=0,
    )
    wt_buf[0:KEY0, :] = gate_rows.astype(BF16)
    finished(w_copies[0])
    start(w_copies[2])
    turn(0)
    finished(p_copies[0:1])
    start(p_copies[2:3])
    finished(w_copies[1])
    start(w_copies[3])
    chunk_dot(0)
    turn(1)
    finished(p_copies[1:2])
    start(p_copies[3:4])
    finished(w_copies[2])
    start(s_copies[1][:2])
    chunk_dot(1)
    turn(2)
    finished(p_copies[2:3])
    start(s_copies[1][2:])
    finished(w_copies[3])
    finished(hp_copies)
    start(s_copies[2][:2])
    chunk_dot(2)
    turn(3)

    edge = jnp.dot(hp_buf[...], wk_buf[...], preferred_element_type=F32).astype(BF16).astype(F32)
    zero4 = jnp.zeros((4, 128), F32)
    h_send[0] = jnp.concatenate(
        [edge[16 * s + 15 : 16 * s + 16] for s in range(seqs)] + [zero4], axis=0
    )
    h_send[1] = jnp.concatenate(
        [edge[16 * s : 16 * s + 1] for s in range(seqs)] + [zero4], axis=0
    )

    pl.semaphore_wait(barrier, sp_n - 1 + tp_n - 1)
    halo_copies = []
    for side, d in ((0, 1), (1, sp_n - 1)):
        copy = pltpu.make_async_remote_copy(
            src_ref=h_send.at[side],
            dst_ref=h_recv.at[side],
            send_sem=h_ssem.at[side],
            recv_sem=h_rsem.at[side],
            device_id=(sp_peer(d), tp),
            device_id_type=MESH_ID,
        )
        copy.start()
        halo_copies.append(copy)

    finished(p_copies[3:4])
    start(s_copies[2][2:])
    chunk_dot(3)

    finished(small_copies[2:])
    for s in range(seqs):
        rows = pl.ds(s, 1)
        par_buf[0, rows, :] = jnp.concatenate(
            [query_v[s, 0:1, :].astype(F32), query_v[s, 1:2, :].astype(F32)], axis=1
        )
        par_buf[1, rows, :] = jnp.concatenate(
            [key_v[s, 0:1, :].astype(F32), key_v[s, 1:2, :].astype(F32)], axis=1
        )
        par_buf[2, rows, :] = halves(nin_v[0:1, s : s + 1], nin_v[1:2, s : s + 1])
        par_buf[3, rows, :] = halves(nfg_v[0:1, s : s + 1], nfg_v[1:2, s : s + 1])
    tap_cols = jnp.transpose(
        jnp.concatenate([taps_v[...].astype(F32), jnp.zeros((5, 128), F32)], axis=0)
    )
    q_cols = jnp.transpose(
        jnp.concatenate([par_buf[0, 0:4, :], jnp.zeros((4, 128), F32)], axis=0)
    )
    bias_col = jnp.where(
        lax.broadcasted_iota(jnp.int32, (2, 1), 0) == 0, bias_v[0], bias_v[1]
    )

    cols_of = out_w.shape[2] // sp_n

    def ow_slot(ref):
        return ref.at[sp // 8, :, lax.rem(sp, 8)]

    def ow_cols(j):
        return out_w.at[:, :, pl.ds(pl.multiple_of(j * cols_of, cols_of), cols_of)]

    def edges():
        for copy in halo_copies:
            copy.wait_recv()
        before = jnp.where(sp == 0, 0.0, jnp.transpose(h_recv[0]))
        after = jnp.where(sp == sp_n - 1, 0.0, jnp.transpose(h_recv[1]))
        return before, after

    pos = lax.broadcasted_iota(jnp.int32, (1, length), 1)
    my_rows = pl.multiple_of(8 * sp, 8)

    def slot_rows(s):
        return pl.ds(pl.multiple_of((s * sp_n + sp) * 8, 8), 8)

    def rows_of(x):
        parts = [part.astype(F32) for part in three_parts(x)]
        return jnp.concatenate(parts + [jnp.zeros((10, length), F32)], axis=0).astype(BF16)

    def finish(s, before, after):
        in_pre = r_buf[s, 0:2, :].astype(BF16).astype(F32)
        fg_pre = r_buf[s, 8:10, :].astype(BF16).astype(F32)
        log_f = log_sigmoid(fg_pre + bias_col) + extra_v[s]
        sums = jnp.dot(rows_of(log_f), tri_buf[...], preferred_element_type=F32)
        later = sums[0:2] + sums[2:4] + sums[4:6]
        total = later[:, 0:1] + log_f[:, 0:1]
        gate = in_pre + later
        top = jnp.max(gate, axis=1, keepdims=True)
        scale = jnp.exp(gate - top)

        key = r_buf[s, KEY0:VAL0, :].astype(BF16).astype(F32)
        earlier = jnp.where(pos == 0, before[:, s : s + 1], pltpu.roll(key, 1, 1))
        coming = jnp.where(pos == length - 1, after[:, s : s + 1], pltpu.roll(key, length - 1, 1))
        mixed = tap_cols[:, 0:1] * earlier + tap_cols[:, 1:2] * key + tap_cols[:, 2:3] * coming
        key_rows = (mixed * jax.nn.sigmoid(mixed) * 0.125).astype(BF16)
        prod = key_rows.astype(F32) * q_cols[:, s : s + 1]
        along = jnp.concatenate(
            [
                jnp.sum(prod[0:64], axis=0, keepdims=True),
                jnp.sum(prod[64:128], axis=0, keepdims=True),
            ],
            axis=0,
        )
        value = r_buf[s, VAL0:, :].astype(BF16).astype(F32)
        weighted = jnp.concatenate(
            [
                (value[0:128] * scale[0:1]).astype(BF16),
                (value[128:256] * scale[1:2]).astype(BF16),
            ],
            axis=0,
        )

        norm_parts = lax.dot_general(rows_of(scale), key_rows, NT, preferred_element_type=F32)
        num_parts = lax.dot_general(rows_of(along), weighted, NT, preferred_element_type=F32)
        outer = lax.dot_general(weighted, key_rows, NT, preferred_element_type=F32)
        mem_buf[pl.ds(128 * s, 128), :] = halves(outer[0:128], outer[128:256])

        def joined(x, h):
            return x[h : h + 1] + x[2 + h : 3 + h] + x[4 + h : 5 + h]

        norm = halves(joined(norm_parts, 0), joined(norm_parts, 1))
        num0 = joined(num_parts, 0)[:, 0:128]
        num1 = joined(num_parts, 1)[:, 128:256]
        num_a = halves(num0, pltpu.roll(num1, 64, 1))
        num_b = halves(pltpu.roll(num0, 64, 1), num1)

        fresh = value_v[s].astype(F32)
        spread = jnp.concatenate([fresh, jnp.zeros((2, 120), F32)], axis=1)
        left = pltpu.roll(spread, 8 * lax.rem(sp, 8), 1)
        fresh_row = halves(left[0:1], pltpu.roll(left[1:2], 64, 1))
        fresh_a = jnp.where(sp < 8, fresh_row, 0.0)
        fresh_b = jnp.where(sp < 8, 0.0, fresh_row)
        tile = jnp.concatenate(
            [
                norm,
                halves(total[0:1], total[1:2]),
                halves(top[0:1], top[1:2]),
                num_a,
                num_b,
                fresh_a,
                fresh_b,
                jnp.zeros((1, 128), F32),
            ],
            axis=0,
        )
        e_buf[pl.ds(8 * s, 8), :] = tile
        e_recv[slot_rows(s), :] = tile
        m_recv[slot_rows(s), :] = mem_buf[pl.ds(128 * s + my_rows, 8), :]

    def send(s):
        @pl.loop(1, sp_n)
        def _(d):
            pltpu.make_async_remote_copy(
                src_ref=e_buf.at[pl.ds(8 * s, 8), :],
                dst_ref=e_recv.at[slot_rows(s), :],
                send_sem=e_ssem.at[s],
                recv_sem=e_rsem.at[s],
                device_id=(sp_peer(d), tp),
                device_id_type=MESH_ID,
            ).start()

        @pl.loop(1, sp_n)
        def _(d):
            j = sp_peer(d)
            pltpu.make_async_remote_copy(
                src_ref=mem_buf.at[pl.ds(pl.multiple_of(128 * s + 8 * j, 8), 8), :],
                dst_ref=m_recv.at[slot_rows(s), :],
                send_sem=m_ssem.at[s],
                recv_sem=m_rsem.at[s],
                device_id=(j, tp),
                device_id_type=MESH_ID,
            ).start()

    def half_dot(s, half):
        rows = pl.ds(half * (length // 2), length // 2)
        r_buf[s, :, rows] = lax.dot_general(
            wt_buf[...], p_buf[s, rows, :], NT, preferred_element_type=F32
        )

    finished(s_copies[1])
    start(s_copies[3])
    half_dot(1, 0)
    half_dot(1, 1)
    own_ow = pltpu.make_async_copy(ow_cols(sp), ow_slot(ow_recv), ow_local)
    own_ow.start()

    @pl.loop(1, sp_n)
    def _(d):
        j = sp_peer(d)
        pltpu.make_async_remote_copy(
            src_ref=ow_cols(j),
            dst_ref=ow_slot(ow_recv),
            send_sem=ow_ssem,
            recv_sem=ow_rsem,
            device_id=(j, tp),
            device_id_type=MESH_ID,
        ).start()

    finished(s_copies[2])
    before, after = edges()
    half_dot(2, 0)
    finish(0, before, after)
    half_dot(2, 1)
    send(0)
    finished(s_copies[3])
    half_dot(3, 0)
    finish(1, before, after)
    finish(2, before, after)
    half_dot(3, 1)
    send(1)
    send(2)
    finish(3, before, after)
    send(3)

    def take(ref, sem, count):
        view = ref.at[pl.ds(0, count), :]
        pltpu.make_async_copy(view, view, sem).wait()

    own_ow.wait()

    row16 = lax.broadcasted_iota(jnp.int32, (sp_n, 128), 0)
    reads, factors = [], []
    for s in range(seqs):
        take(e_recv, e_rsem.at[s], 8 * (sp_n - 1))
    for s in range(seqs):

        def rows_at(k):
            return e_recv[pl.ds(s * sp_n * 8 + k, sp_n, stride=8), :]

        later = jnp.where(row16 < sp_n - 1, pltpu.roll(rows_at(1), sp_n - 1, 0), 0.0)
        shift = 1
        while shift < sp_n:
            later = later + jnp.where(
                row16 < sp_n - shift, pltpu.roll(later, sp_n - shift, 0), 0.0
            )
            shift *= 2
        gate = rows_at(2) + later
        peak = jnp.max(gate, axis=0, keepdims=True)
        factor = jnp.exp(gate - peak)
        factors.append(factor)

        def summed(k):
            return jnp.sum(factor * rows_at(k), axis=0, keepdims=True)

        norm, num_a, num_b = summed(0), summed(3), summed(4)
        fresh_a = jnp.sum(rows_at(5), axis=0, keepdims=True)
        fresh_b = jnp.sum(rows_at(6), axis=0, keepdims=True)
        q, k = par_buf[0, s : s + 1, :], par_buf[1, s : s + 1, :]
        gate_in, gate_fg = par_buf[2, s : s + 1, :], par_buf[3, s : s + 1, :]
        kept = log_sigmoid(gate_fg) + peak
        new_peak = jnp.maximum(kept, gate_in)
        old_scale = jnp.exp(kept - new_peak)
        new_scale = jnp.exp(gate_in - new_peak)

        def by_head(x):
            left = jnp.sum(jnp.where(first_head, x, 0.0), axis=1, keepdims=True)
            right = jnp.sum(jnp.where(first_head, 0.0, x), axis=1, keepdims=True)
            return halves(left, right)

        denom = jnp.maximum(jnp.abs(by_head(q * (old_scale * norm + new_scale * k))), 1.0)
        fresh_scale = new_scale * by_head(q * k)
        read_a = (old_scale * num_a + fresh_scale * fresh_a) / denom
        read_b = (old_scale * num_b + fresh_scale * fresh_b) / denom
        reads.append(jnp.concatenate([read_a, read_b], axis=1))
        mine = pltpu.roll(norm, lax.rem(128 - 4 * sp, 128), 1)
        packed[32 + s : 33 + s, :] = mine
        packed[36 + s : 37 + s, :] = peak

    ow_words = pltpu.make_async_copy(
        out_w.at[:, :, pl.ds(0, cols_of * (sp_n - 1))],
        out_w.at[:, :, pl.ds(0, cols_of * (sp_n - 1))],
        ow_rsem,
    )
    ow_words.wait()
    read = jnp.concatenate(reads + [jnp.zeros((12, 256), F32)], axis=0).astype(BF16)
    weight = ow_recv[...].reshape(256, cols_of)
    part = jnp.dot(read, weight, preferred_element_type=F32)[0:8]
    part_buf[...] = part
    part_recv[tp] = part

    @pl.loop(1, tp_n)
    def _(d):
        pltpu.make_async_remote_copy(
            src_ref=part_buf,
            dst_ref=part_recv.at[tp],
            send_sem=o_ssem,
            recv_sem=o_rsem,
            device_id=(sp, tp_peer(d)),
            device_id_type=MESH_ID,
        ).start()

    for s in range(seqs):
        take(m_recv, m_rsem.at[s], 8 * (sp_n - 1))
    for s in range(seqs):
        memory = jnp.zeros((8, 128), F32)
        for i in range(sp_n):
            base = (s * sp_n + i) * 8
            memory = memory + factors[s][i : i + 1] * m_recv[base : base + 8, :]
        packed[8 * s : 8 * s + 8, :] = memory

    view = part_recv.at[pl.ds(0, tp_n - 1)]
    pltpu.make_async_copy(view, view, o_rsem).wait()
    whole = part_recv[0]
    for i in range(1, tp_n):
        whole = whole + part_recv[i]
    turned = pltpu.roll(whole, lax.rem(cols_of - 32 * tp, cols_of), 1)
    packed[40:48, :] = turned[:, 0:128]

    for copy in halo_copies:
        copy.wait_send()
    pltpu.make_async_copy(
        out_w.at[:, :, pl.ds(0, cols_of * (sp_n - 1))],
        out_w.at[:, :, pl.ds(0, cols_of * (sp_n - 1))],
        ow_ssem,
    ).wait()
    for s in range(seqs):
        take(e_recv, e_ssem.at[s], 8 * (sp_n - 1))
        take(m_recv, m_ssem.at[s], 8 * (sp_n - 1))
    pltpu.make_async_copy(view, view, o_ssem).wait()


def unpack(packed, mem_out, norm_out, peak_out, read_out):
    seqs = mem_out.shape[0]
    for s in range(seqs):
        rows = packed[8 * s : 8 * s + 8, :]
        mem_out[s, 0] = rows[:, 0:64].astype(BF16)
        mem_out[s, 1] = rows[:, 64:128].astype(BF16)
        norm = packed[32 + s : 33 + s, :]
        norm_out[s, 0:1, :] = norm[:, 0:4].astype(BF16)
        norm_out[s, 1:2, :] = norm[:, 64:68].astype(BF16)
        peak = packed[36 + s : 37 + s, :]
        peak_out[0:1, s : s + 1] = peak[:, 0:1]
        peak_out[1:2, s : s + 1] = peak[:, 64:65]
    read_out[...] = packed[40:44, 0:32].astype(BF16)


def body(
    prompt, key_weight, value_weight, input_gate_weight, forget_gate_weight, forget_bias,
    key_taps, extra_decay, new_query, new_key, new_value, new_input_gate, new_forget_gate,
    out_weight,
):
    seqs, length, width = prompt.shape
    sp_n = lax.axis_size("sp")
    tp_n = lax.axis_size("tp")
    cols_of = out_weight.shape[2] // sp_n
    any_spec = pl.BlockSpec(memory_space=pl.ANY)
    vmem = pl.BlockSpec(memory_space=pltpu.VMEM)
    dma = pltpu.SemaphoreType.DMA
    packed = pl.pallas_call(
        kernel,
        out_shape=pltpu.VMEM((48, 128), F32),
        in_specs=[any_spec] * 14,
        out_specs=vmem,
        scratch_shapes=[
            pltpu.VMEM((seqs, length, width), BF16),
            pltpu.VMEM((width, 128), BF16),
            pltpu.VMEM((width, 256), BF16),
            pltpu.VMEM((400, width), BF16),
            pltpu.VMEM((64, width), BF16),
            pltpu.VMEM((seqs, 400, length), F32),
            pltpu.VMEM((length, length), BF16),
            pltpu.VMEM((4, 8, 128), F32),
            pltpu.VMEM((seqs * 128, 128), F32),
            pltpu.VMEM((seqs * 8, 128), F32),
            pltpu.VMEM((2, 8, 128), F32),
            pltpu.VMEM((2, 8, 128), F32),
            pltpu.VMEM((seqs * sp_n * 8, 128), F32),
            pltpu.VMEM((seqs * sp_n * 8, 128), F32),
            pltpu.VMEM((2, 2, 8, 8, cols_of), BF16),
            pltpu.VMEM((8, cols_of), F32),
            pltpu.VMEM((tp_n, 8, cols_of), F32),
            pltpu.VMEM((2, width), BF16),
            pltpu.VMEM((2, width), BF16),
            pltpu.SMEM((2,), F32),
            pltpu.VMEM((3, 128), BF16),
            pltpu.VMEM((seqs, 2, length), F32),
            pltpu.VMEM((seqs, 2, 64), BF16),
            pltpu.VMEM((seqs, 2, 64), BF16),
            pltpu.VMEM((seqs, 2, 8), BF16),
            pltpu.VMEM((2, seqs), F32),
            pltpu.VMEM((2, seqs), F32),
            dma((2, CHUNKS)),
            dma((seqs, CHUNKS)),
            dma((2 * seqs,)),
            dma((10,)),
            dma,
            dma((2,)),
            dma((2,)),
            dma((seqs,)),
            dma((seqs,)),
            dma((seqs,)),
            dma((seqs,)),
            dma,
            dma,
            dma,
            dma,
        ],
        compiler_params=pltpu.CompilerParams(
            collective_id=0, has_side_effects=True, vmem_limit_bytes=60 * 1024 * 1024
        ),
        name="prompt_state",
    )(
        prompt,
        key_weight,
        value_weight,
        input_gate_weight.T,
        forget_gate_weight.T,
        forget_bias,
        key_taps,
        jnp.transpose(extra_decay, (0, 2, 1)),
        new_query,
        new_key,
        new_value,
        new_input_gate.T,
        new_forget_gate.T,
        out_weight,
    )
    memory, norm, peak, read = pl.pallas_call(
        unpack,
        out_shape=(
            jax.ShapeDtypeStruct((seqs, 2, 8, 64), BF16),
            jax.ShapeDtypeStruct((seqs, 2, 4), BF16),
            jax.ShapeDtypeStruct((2, seqs), F32),
            jax.ShapeDtypeStruct((seqs, 32), BF16),
        ),
        in_specs=[vmem],
        out_specs=(vmem,) * 4,
        compiler_params=pltpu.CompilerParams(vmem_limit_bytes=1024 * 1024),
        name="unpack",
    )(packed)
    return jnp.transpose(memory, (0, 1, 3, 2)), norm, peak.T, read


def solution(mesh):
    in_specs = (
        P(None, "sp", None),
        P(None, "tp"),
        P(None, "tp"),
        P(None, "tp"),
        P(None, "tp"),
        P("tp"),
        P(None, "tp"),
        P(None, "sp", "tp"),
        P(None, "tp", None),
        P(None, "tp", None),
        P(None, "tp", "sp"),
        P(None, "tp"),
        P(None, "tp"),
        P("tp", "sp", None),
    )
    out_specs = (
        P(None, "tp", None, "sp"),
        P(None, "tp", "sp"),
        P(None, "tp"),
        P(None, ("sp", "tp")),
    )
    return jax.shard_map(body, mesh=mesh, in_specs=in_specs, out_specs=out_specs, check_vma=False)
```

```python
import jax
import jax.numpy as jnp
from jax import lax
from jax.experimental import pallas as pl
from jax.experimental.pallas import tpu as pltpu
from jax.sharding import PartitionSpec as P

MESH_ID = pl.DeviceIdType.MESH
F32 = jnp.float32
BF16 = jnp.bfloat16
NT = (((1,), (1,)), ((), ()))
KEY0 = 16
VAL0 = 144
CHUNKS = 4


def log_sigmoid(x):
    return jnp.minimum(x, 0.0) - jnp.log1p(jnp.exp(-jnp.abs(x)))


def three_parts(x):
    high = x.astype(BF16)
    rest = x - high.astype(F32)
    middle = rest.astype(BF16)
    low = (rest - middle.astype(F32)).astype(BF16)
    return high, middle, low


def kernel(
    prompt, key_w, value_w, in_w, fg_w, fg_bias, taps, extra, query, new_key, new_value,
    new_in, new_fg, out_w,
    packed,
    p_buf, wk_buf, wv_buf, wt_buf, hp_buf, r_buf, tri_buf, par_buf, mem_buf, e_buf,
    h_send, h_recv, e_recv, m_recv, ow_recv, part_buf, part_recv, f_buf, f_recv, lhs_buf, key_buf,
    along_buf, suf_buf, ow_buf, col_buf,
    in_v, fg_v, bias_v, taps_v, extra_v, query_v, key_v, value_v, nin_v, nfg_v,
    w_sem, p_sem, hp_sem, small_sem, ow_local, h_ssem, h_rsem, e_ssem, e_rsem, m_ssem, m_rsem,
    ow_ssem, ow_rsem, o_ssem, o_rsem, f_ssem, f_rsem,
):
    seqs, length, width = p_buf.shape
    sp_n, tp_n = lax.axis_size("sp"), lax.axis_size("tp")
    sp, tp = lax.axis_index("sp"), lax.axis_index("tp")
    step = width // CHUNKS

    barrier = pltpu.get_barrier_semaphore()

    def sp_peer(d):
        return lax.rem(sp + d, sp_n)

    def tp_peer(d):
        return lax.rem(tp + d, tp_n)

    small_pairs = (
        (in_w, in_v), (fg_w, fg_v), (fg_bias, bias_v), (taps, taps_v), (extra, extra_v),
        (query, query_v), (new_key, key_v), (new_value, value_v), (new_in, nin_v),
        (new_fg, nfg_v),
    )
    small_copies = [
        pltpu.make_async_copy(src, dst, small_sem.at[i])
        for i, (src, dst) in enumerate(small_pairs)
    ]
    hp_copies = []
    for s in range(seqs):
        for side, row in ((0, 0), (1, length - 8)):
            g = 2 * s + side
            hp_copies.append(
                pltpu.make_async_copy(
                    prompt.at[s, pl.ds(row, 8), :], hp_buf.at[pl.ds(8 * g, 8), :], hp_sem.at[g]
                )
            )
    wk_copies = [
        pltpu.make_async_copy(key_w.at[rows, :], wk_buf.at[rows, :], w_sem.at[0, i])
        for i, rows in enumerate((pl.ds(0, width // 2), pl.ds(width // 2, width // 2)))
    ]
    w_copies, p_copies = [], []
    for c in range(CHUNKS):
        rows = pl.ds(c * step, step)
        w_copies.append(
            pltpu.make_async_copy(value_w.at[rows, :], wv_buf.at[rows, :], w_sem.at[1, c])
        )
        p_copies.append(
            pltpu.make_async_copy(prompt.at[0, :, rows], p_buf.at[0, :, rows], p_sem.at[0, c])
        )
    s_copies = [p_copies]
    for s in range(1, seqs):
        group = []
        for c in range(CHUNKS):
            cols = pl.ds(c * step, step)
            group.append(
                pltpu.make_async_copy(prompt.at[s, :, cols], p_buf.at[s, :, cols], p_sem.at[s, c])
            )
        s_copies.append(group)

    def start(copies):
        for copy in copies:
            copy.start()

    def finished(copies):
        for copy in copies:
            copy.wait()

    start(wk_copies)
    start(hp_copies)
    start(w_copies[:1])
    start(p_copies[:1])
    start(small_copies)
    start(w_copies[1:2])
    start(p_copies[1:2])

    @pl.loop(1, sp_n)
    def _(d):
        pl.semaphore_signal(barrier, inc=1, device_id=(sp_peer(d), tp), device_id_type=MESH_ID)

    @pl.loop(1, tp_n)
    def _(d):
        pl.semaphore_signal(barrier, inc=1, device_id=(sp, tp_peer(d)), device_id_type=MESH_ID)

    tri_buf[...] = (
        lax.broadcasted_iota(jnp.int32, (length, length), 0)
        > lax.broadcasted_iota(jnp.int32, (length, length), 1)
    ).astype(F32).astype(BF16)

    lane = lax.broadcasted_iota(jnp.int32, (1, 128), 1)
    first_head = lane < 64

    def halves(left, right):
        return jnp.where(first_head, left, right)

    def chunk_of(c):
        return pl.ds(c * step, step)

    def turn(c):
        cols = chunk_of(c)
        wt_buf[VAL0:, cols] = jnp.transpose(wv_buf[cols, :])

    def chunk_dot(s, c):
        cols = chunk_of(c)
        part = lax.dot_general(
            wt_buf[:, cols], p_buf[s, :, cols], NT, preferred_element_type=F32
        )
        if c == 0:
            r_buf[s] = part
        else:
            r_buf[s] = r_buf[s] + part

    finished(wk_copies)
    start(w_copies[2:])
    start(p_copies[2:])
    for c in range(CHUNKS):
        cols = chunk_of(c)
        wt_buf[KEY0:VAL0, cols] = jnp.transpose(wk_buf[cols, :])
    finished(hp_copies)

    edge = jnp.dot(hp_buf[...], wk_buf[...], preferred_element_type=F32).astype(BF16).astype(F32)
    zero4 = jnp.zeros((4, 128), F32)
    h_send[0] = jnp.concatenate(
        [edge[16 * s + 15 : 16 * s + 16] for s in range(seqs)] + [zero4], axis=0
    )
    h_send[1] = jnp.concatenate(
        [edge[16 * s : 16 * s + 1] for s in range(seqs)] + [zero4], axis=0
    )

    finished(small_copies)
    gate_rows = jnp.concatenate(
        [
            in_v[...].astype(F32), jnp.zeros((6, width), F32),
            fg_v[...].astype(F32), jnp.zeros((6, width), F32),
        ],
        axis=0,
    )
    wt_buf[0:KEY0, :] = gate_rows.astype(BF16)
    finished(w_copies[:1])
    start(s_copies[1][:2])
    turn(0)
    finished(p_copies[:1])
    finished(w_copies[1:2])
    start(s_copies[1][2:])
    chunk_dot(0, 0)
    turn(1)
    pl.semaphore_wait(barrier, sp_n - 1 + tp_n - 1)
    halo_copies = []
    for side, d in ((0, 1), (1, sp_n - 1)):
        copy = pltpu.make_async_remote_copy(
            src_ref=h_send.at[side],
            dst_ref=h_recv.at[side],
            send_sem=h_ssem.at[side],
            recv_sem=h_rsem.at[side],
            device_id=(sp_peer(d), tp),
            device_id_type=MESH_ID,
        )
        copy.start()
        halo_copies.append(copy)

    finished(p_copies[1:2])
    finished(w_copies[2:3])
    chunk_dot(0, 1)
    turn(2)
    finished(p_copies[2:3])
    finished(w_copies[3:])
    start(s_copies[2][:2])
    chunk_dot(0, 2)
    turn(3)

    for s in range(seqs):
        rows = pl.ds(s, 1)
        par_buf[0, rows, :] = jnp.concatenate(
            [query_v[s, 0:1, :].astype(F32), query_v[s, 1:2, :].astype(F32)], axis=1
        )
        par_buf[1, rows, :] = jnp.concatenate(
            [key_v[s, 0:1, :].astype(F32), key_v[s, 1:2, :].astype(F32)], axis=1
        )
        par_buf[2, rows, :] = halves(nin_v[0:1, s : s + 1], nin_v[1:2, s : s + 1])
        par_buf[3, rows, :] = halves(nfg_v[0:1, s : s + 1], nfg_v[1:2, s : s + 1])
        fresh = value_v[s].astype(F32)
        spread = jnp.concatenate([fresh, jnp.zeros((2, 120), F32)], axis=1)
        left = pltpu.roll(spread, 8 * lax.rem(sp, 8), 1)
        fresh_row = halves(left[0:1], pltpu.roll(left[1:2], 64, 1))
        f_buf[s : s + 1, :] = jnp.where(sp < 8, fresh_row, 0.0)
        f_buf[4 + s : 5 + s, :] = jnp.where(sp < 8, 0.0, fresh_row)
    col_buf[:, 0:8] = jnp.transpose(
        jnp.concatenate(
            [taps_v[...].astype(F32), jnp.zeros((1, 128), F32), par_buf[0, 0:4, :]], axis=0
        )
    )

    bias_col = jnp.where(
        lax.broadcasted_iota(jnp.int32, (2, 1), 0) == 0, bias_v[0], bias_v[1]
    )

    cols_of = out_w.shape[2] // sp_n

    def ow_slot(ref):
        return ref.at[sp // 8, :, lax.rem(sp, 8)]

    def ow_cols(j):
        return out_w.at[:, :, pl.ds(pl.multiple_of(j * cols_of, cols_of), cols_of)]

    pos = lax.broadcasted_iota(jnp.int32, (1, length), 1)
    my_rows = pl.multiple_of(8 * sp, 8)
    my_tile = pl.multiple_of(8 * sp, 8)

    def slot_rows(s, size):
        return pl.ds(pl.multiple_of((s * sp_n + sp) * size, size), size)

    def rows_of(x):
        parts = [part.astype(F32) for part in three_parts(x)]
        return jnp.concatenate(parts + [jnp.zeros((10, length), F32)], axis=0).astype(BF16)

    def joined(x, h):
        return x[h : h + 1] + x[2 + h : 3 + h] + x[4 + h : 5 + h]

    def suffix(s):
        fg_pre = r_buf[s, 8:10, :].astype(BF16).astype(F32)
        log_f = log_sigmoid(fg_pre + bias_col) + extra_v[s]
        sums = jnp.dot(rows_of(log_f), tri_buf[...], preferred_element_type=F32)
        later = sums[0:2] + sums[2:4] + sums[4:6]
        suf_buf[s, 0:2, :] = later
        suf_buf[s, 2:4, :] = jnp.broadcast_to(later[:, 0:1] + log_f[:, 0:1], (2, length))

    def keys(s):
        key = r_buf[s, KEY0:VAL0, :].astype(BF16).astype(F32)
        earlier = jnp.where(pos == 0, col_buf[:, 8 + s : 9 + s], pltpu.roll(key, 1, 1))
        coming = jnp.where(
            pos == length - 1, col_buf[:, 16 + s : 17 + s], pltpu.roll(key, length - 1, 1)
        )
        mixed = col_buf[:, 0:1] * earlier + col_buf[:, 1:2] * key + col_buf[:, 2:3] * coming
        key_rows = (mixed * jax.nn.sigmoid(mixed) * 0.125).astype(BF16)
        key_buf[s] = key_rows
        prod = key_rows.astype(F32) * col_buf[:, 4 + s : 5 + s]
        along = jnp.concatenate(
            [
                jnp.sum(prod[0:64], axis=0, keepdims=True),
                jnp.sum(prod[64:128], axis=0, keepdims=True),
            ],
            axis=0,
        )
        along_buf[s] = rows_of(along)

    def weigh(s):
        in_pre = r_buf[s, 0:2, :].astype(BF16).astype(F32)
        gate = in_pre + suf_buf[s, 0:2, :]
        top = jnp.max(gate, axis=1, keepdims=True)
        scale = jnp.exp(gate - top)
        lhs_buf[s, 0:16, :] = rows_of(scale)
        for h in range(2):
            value = r_buf[s, VAL0 + 128 * h : VAL0 + 128 * (h + 1), :].astype(BF16).astype(F32)
            lhs_buf[s, 16 + 128 * h : 144 + 128 * h, :] = (value * scale[h : h + 1]).astype(BF16)
        total = suf_buf[s, 2:4, 0:1]
        row = jnp.where(
            lax.rem(lane, 64) < 32,
            halves(total[0:1], total[1:2]),
            halves(top[0:1], top[1:2]),
        )
        e_buf[4 * s + 3 : 4 * s + 4, :] = row

    def outer(s):
        num_parts = lax.dot_general(
            along_buf[s], lhs_buf[s, 16:, :], NT, preferred_element_type=F32
        )
        both = lax.dot_general(lhs_buf[s], key_buf[s], NT, preferred_element_type=F32)
        num0 = joined(num_parts, 0)[:, 0:128]
        num1 = joined(num_parts, 1)[:, 128:256]
        e_buf[4 * s : 4 * s + 1, :] = halves(joined(both, 0), joined(both, 1))
        e_buf[4 * s + 1 : 4 * s + 2, :] = halves(num0, pltpu.roll(num1, 64, 1))
        e_buf[4 * s + 2 : 4 * s + 3, :] = halves(pltpu.roll(num0, 64, 1), num1)
        mem_buf[pl.ds(128 * s, 128), :] = halves(both[16:144], both[144:272])

    z, x = sp // 4, lax.rem(sp, 4)
    offsets = sorted(
        ((dz, dx) for dz in range(4) for dx in range(4) if dz or dx),
        key=lambda o: -(min(o[0], 4 - o[0]) + min(o[1], 4 - o[1])),
    )
    peers = [lax.rem(z + dz, 4) * 4 + lax.rem(x + dx, 4) for dz, dx in offsets]

    def send_sums(s):
        e_recv[slot_rows(s, 4), :] = e_buf[4 * s : 4 * s + 4, :]
        for j in peers:
            pltpu.make_async_remote_copy(
                src_ref=e_buf.at[pl.ds(4 * s, 4), :],
                dst_ref=e_recv.at[slot_rows(s, 4), :],
                send_sem=e_ssem.at[s],
                recv_sem=e_rsem.at[s],
                device_id=(j, tp),
                device_id_type=MESH_ID,
            ).start()

    def send_memory(s):
        m_recv[slot_rows(s, 8), :] = mem_buf[pl.ds(128 * s + my_rows, 8), :]
        for j in peers:
            pltpu.make_async_remote_copy(
                src_ref=mem_buf.at[pl.ds(pl.multiple_of(128 * s + 8 * j, 8), 8), :],
                dst_ref=m_recv.at[slot_rows(s, 8), :],
                send_sem=m_ssem.at[s],
                recv_sem=m_rsem.at[s],
                device_id=(j, tp),
                device_id_type=MESH_ID,
            ).start()

    finished(p_copies[3:])
    start(s_copies[2][2:])
    chunk_dot(0, 3)
    finished(s_copies[1][:2])
    start(s_copies[3])
    chunk_dot(1, 0)
    chunk_dot(1, 1)
    suffix(0)
    finished(s_copies[1][2:])
    chunk_dot(1, 2)
    chunk_dot(1, 3)

    for copy in halo_copies:
        copy.wait_recv()
    finished(s_copies[2])
    finished(s_copies[3])
    col_buf[:, 8:16] = jnp.where(sp == 0, 0.0, jnp.transpose(h_recv[0]))
    col_buf[:, 16:24] = jnp.where(sp == sp_n - 1, 0.0, jnp.transpose(h_recv[1]))
    chunk_dot(2, 0)
    chunk_dot(2, 1)
    suffix(1)
    keys(0)
    weigh(0)

    own_ow = pltpu.make_async_copy(ow_cols(sp), ow_slot(ow_recv), ow_local)
    own_ow.start()
    f_recv[pl.ds(my_tile, 8), :] = f_buf[...]
    for j in peers:
        pltpu.make_async_remote_copy(
            src_ref=f_buf,
            dst_ref=f_recv.at[pl.ds(my_tile, 8), :],
            send_sem=f_ssem,
            recv_sem=f_rsem,
            device_id=(j, tp),
            device_id_type=MESH_ID,
        ).start()
        pltpu.make_async_remote_copy(
            src_ref=ow_cols(j),
            dst_ref=ow_slot(ow_recv),
            send_sem=ow_ssem,
            recv_sem=ow_rsem,
            device_id=(j, tp),
            device_id_type=MESH_ID,
        ).start()

    chunk_dot(2, 2)
    outer(0)
    chunk_dot(2, 3)
    chunk_dot(3, 0)
    keys(1)
    weigh(1)
    send_sums(0)
    send_memory(0)
    suffix(2)
    chunk_dot(3, 1)
    outer(1)
    chunk_dot(3, 2)
    send_sums(1)
    send_memory(1)
    keys(2)
    weigh(2)
    chunk_dot(3, 3)
    outer(2)
    suffix(3)
    send_sums(2)
    keys(3)
    weigh(3)
    outer(3)
    send_sums(3)
    send_memory(2)
    send_memory(3)

    def take(ref, sem, count):
        view = ref.at[pl.ds(0, count), :]
        pltpu.make_async_copy(view, view, sem).wait()

    own_ow.wait()
    ow_bytes = out_w.at[:, :, pl.ds(0, cols_of * (sp_n - 1))]
    pltpu.make_async_copy(ow_bytes, ow_bytes, ow_rsem).wait()
    ow_buf[...] = ow_recv[...].reshape(256, cols_of)
    take(f_recv, f_rsem, 8 * (sp_n - 1))
    fresh_sum = f_recv[0:8, :]
    for i in range(1, sp_n):
        fresh_sum = fresh_sum + f_recv[8 * i : 8 * i + 8, :]

    row16 = lax.broadcasted_iota(jnp.int32, (sp_n, 128), 0)
    low_lanes = lax.rem(lax.broadcasted_iota(jnp.int32, (sp_n, 128), 1), 64) < 32

    def by_head(x):
        left = jnp.sum(jnp.where(first_head, x, 0.0), axis=1, keepdims=True)
        right = jnp.sum(jnp.where(first_head, 0.0, x), axis=1, keepdims=True)
        return halves(left, right)

    def combine(s):
        def rows_at(k):
            return e_recv[pl.ds(s * sp_n * 4 + k, sp_n, stride=4), :]

        stats = rows_at(3)
        totals = jnp.where(low_lanes, stats, pltpu.roll(stats, 32, 1))
        tops = jnp.where(low_lanes, pltpu.roll(stats, 96, 1), stats)
        later = jnp.where(row16 < sp_n - 1, pltpu.roll(totals, sp_n - 1, 0), 0.0)
        shift = 1
        while shift < sp_n:
            later = later + jnp.where(
                row16 < sp_n - shift, pltpu.roll(later, sp_n - shift, 0), 0.0
            )
            shift *= 2
        gate = tops + later
        peak = jnp.max(gate, axis=0, keepdims=True)
        factor = jnp.exp(gate - peak)

        def summed(k):
            return jnp.sum(factor * rows_at(k), axis=0, keepdims=True)

        norm, num_a, num_b = summed(0), summed(1), summed(2)
        q, k = par_buf[0, s : s + 1, :], par_buf[1, s : s + 1, :]
        gate_in, gate_fg = par_buf[2, s : s + 1, :], par_buf[3, s : s + 1, :]
        kept = log_sigmoid(gate_fg) + peak
        new_peak = jnp.maximum(kept, gate_in)
        old_scale = jnp.exp(kept - new_peak)
        new_scale = jnp.exp(gate_in - new_peak)
        denom = jnp.maximum(jnp.abs(by_head(q * (old_scale * norm + new_scale * k))), 1.0)
        fresh_scale = new_scale * by_head(q * k)
        read_a = (old_scale * num_a + fresh_scale * fresh_sum[s : s + 1]) / denom
        read_b = (old_scale * num_b + fresh_scale * fresh_sum[4 + s : 5 + s]) / denom
        packed[32 + s : 33 + s, :] = pltpu.roll(norm, lax.rem(128 - 4 * sp, 128), 1)
        packed[36 + s : 37 + s, :] = peak
        return jnp.concatenate([read_a, read_b], axis=1), factor

    reads, factors = [], []
    for s in range(seqs - 1):
        take(e_recv, e_rsem.at[s], 4 * (sp_n - 1))
        row, factor = combine(s)
        reads.append(row)
        factors.append(factor)
    take(e_recv, e_rsem.at[seqs - 1], 4 * (sp_n - 1))
    row, factor = combine(seqs - 1)
    reads.append(row)
    factors.append(factor)

    read = jnp.concatenate(reads + [jnp.zeros((12, 256), F32)], axis=0).astype(BF16)
    part = jnp.dot(read, ow_buf[...], preferred_element_type=F32)[0:4]
    part_buf[0] = part[:, 0:128]
    part_buf[1] = part[:, 128:256]
    part_recv[tp] = part_buf[tp // 4]
    y, core = tp // 2, lax.rem(tp, 2)
    for dy, dc in ((2, 1), (2, 0), (1, 1), (3, 1), (1, 0), (3, 0), (0, 1)):
        j = lax.rem(y + dy, 4) * 2 + lax.rem(core + dc, 2)
        pltpu.make_async_remote_copy(
            src_ref=part_buf.at[j // 4],
            dst_ref=part_recv.at[tp],
            send_sem=o_ssem,
            recv_sem=o_rsem,
            device_id=(sp, j),
            device_id_type=MESH_ID,
        ).start()

    for s in range(seqs):
        take(m_recv, m_rsem.at[s], 8 * (sp_n - 1))
    for s in range(seqs):
        memory = jnp.zeros((8, 128), F32)
        for i in range(sp_n):
            base = (s * sp_n + i) * 8
            memory = memory + factors[s][i : i + 1] * m_recv[base : base + 8, :]
        packed[8 * s : 8 * s + 8, :] = memory

    view = part_recv.at[pl.ds(0, tp_n - 1)]
    pltpu.make_async_copy(view, view, o_rsem).wait()
    whole = part_recv[0]
    for i in range(1, tp_n):
        whole = whole + part_recv[i]
    packed[40:44, :] = pltpu.roll(whole, lax.rem(128 - 32 * lax.rem(tp, 4), 128), 1)

    for copy in halo_copies:
        copy.wait_send()
    pltpu.make_async_copy(ow_bytes, ow_bytes, ow_ssem).wait()
    take(f_recv, f_ssem, 8 * (sp_n - 1))
    for s in range(seqs):
        take(e_recv, e_ssem.at[s], 4 * (sp_n - 1))
        take(m_recv, m_ssem.at[s], 8 * (sp_n - 1))
    pltpu.make_async_copy(view, view, o_ssem).wait()


def unpack(packed, mem_out, norm_out, peak_out, read_out):
    seqs = mem_out.shape[0]
    for s in range(seqs):
        rows = packed[8 * s : 8 * s + 8, :]
        mem_out[s, 0] = rows[:, 0:64].astype(BF16)
        mem_out[s, 1] = rows[:, 64:128].astype(BF16)
        norm = packed[32 + s : 33 + s, :]
        norm_out[s, 0:1, :] = norm[:, 0:4].astype(BF16)
        norm_out[s, 1:2, :] = norm[:, 64:68].astype(BF16)
        peak = packed[36 + s : 37 + s, :]
        peak_out[0:1, s : s + 1] = peak[:, 0:1]
        peak_out[1:2, s : s + 1] = peak[:, 64:65]
    read_out[...] = packed[40:44, 0:32].astype(BF16)


def body(
    prompt, key_weight, value_weight, input_gate_weight, forget_gate_weight, forget_bias,
    key_taps, extra_decay, new_query, new_key, new_value, new_input_gate, new_forget_gate,
    out_weight,
):
    seqs, length, width = prompt.shape
    sp_n = lax.axis_size("sp")
    tp_n = lax.axis_size("tp")
    cols_of = out_weight.shape[2] // sp_n
    any_spec = pl.BlockSpec(memory_space=pl.ANY)
    vmem = pl.BlockSpec(memory_space=pltpu.VMEM)
    dma = pltpu.SemaphoreType.DMA
    packed = pl.pallas_call(
        kernel,
        out_shape=pltpu.VMEM((48, 128), F32),
        in_specs=[any_spec] * 14,
        out_specs=vmem,
        scratch_shapes=[
            pltpu.VMEM((seqs, length, width), BF16),
            pltpu.VMEM((width, 128), BF16),
            pltpu.VMEM((width, 256), BF16),
            pltpu.VMEM((400, width), BF16),
            pltpu.VMEM((64, width), BF16),
            pltpu.VMEM((seqs, 400, length), F32),
            pltpu.VMEM((length, length), BF16),
            pltpu.VMEM((4, 8, 128), F32),
            pltpu.VMEM((seqs * 128, 128), F32),
            pltpu.VMEM((seqs * 4, 128), F32),
            pltpu.VMEM((2, 8, 128), F32),
            pltpu.VMEM((2, 8, 128), F32),
            pltpu.VMEM((seqs * sp_n * 4, 128), F32),
            pltpu.VMEM((seqs * sp_n * 8, 128), F32),
            pltpu.VMEM((2, 2, 8, 8, cols_of), BF16),
            pltpu.VMEM((2, 4, 128), F32),
            pltpu.VMEM((tp_n, 4, 128), F32),
            pltpu.VMEM((8, 128), F32),
            pltpu.VMEM((sp_n * 8, 128), F32),
            pltpu.VMEM((seqs, 272, length), BF16),
            pltpu.VMEM((seqs, 128, length), BF16),
            pltpu.VMEM((seqs, 16, length), BF16),
            pltpu.VMEM((seqs, 4, length), F32),
            pltpu.VMEM((256, cols_of), BF16),
            pltpu.VMEM((128, 128), F32),
            pltpu.VMEM((2, width), BF16),
            pltpu.VMEM((2, width), BF16),
            pltpu.SMEM((2,), F32),
            pltpu.VMEM((3, 128), BF16),
            pltpu.VMEM((seqs, 2, length), F32),
            pltpu.VMEM((seqs, 2, 64), BF16),
            pltpu.VMEM((seqs, 2, 64), BF16),
            pltpu.VMEM((seqs, 2, 8), BF16),
            pltpu.VMEM((2, seqs), F32),
            pltpu.VMEM((2, seqs), F32),
            dma((2, CHUNKS)),
            dma((seqs, CHUNKS)),
            dma((2 * seqs,)),
            dma((10,)),
            dma,
            dma((2,)),
            dma((2,)),
            dma((seqs,)),
            dma((seqs,)),
            dma((seqs,)),
            dma((seqs,)),
            dma,
            dma,
            dma,
            dma,
            dma,
            dma,
        ],
        compiler_params=pltpu.CompilerParams(
            collective_id=0, has_side_effects=True, vmem_limit_bytes=60 * 1024 * 1024
        ),
        name="prompt_state",
    )(
        prompt,
        key_weight,
        value_weight,
        input_gate_weight.T,
        forget_gate_weight.T,
        forget_bias,
        key_taps,
        jnp.transpose(extra_decay, (0, 2, 1)),
        new_query,
        new_key,
        new_value,
        new_input_gate.T,
        new_forget_gate.T,
        out_weight,
    )
    memory, norm, peak, read = pl.pallas_call(
        unpack,
        out_shape=(
            jax.ShapeDtypeStruct((seqs, 2, 8, 64), BF16),
            jax.ShapeDtypeStruct((seqs, 2, 4), BF16),
            jax.ShapeDtypeStruct((2, seqs), F32),
            jax.ShapeDtypeStruct((seqs, 32), BF16),
        ),
        in_specs=[vmem],
        out_specs=(vmem,) * 4,
        compiler_params=pltpu.CompilerParams(vmem_limit_bytes=1024 * 1024),
        name="unpack",
    )(packed)
    return jnp.transpose(memory, (0, 1, 3, 2)), norm, peak.T, read


def solution(mesh):
    in_specs = (
        P(None, "sp", None),
        P(None, "tp"),
        P(None, "tp"),
        P(None, "tp"),
        P(None, "tp"),
        P("tp"),
        P(None, "tp"),
        P(None, "sp", "tp"),
        P(None, "tp", None),
        P(None, "tp", None),
        P(None, "tp", "sp"),
        P(None, "tp"),
        P(None, "tp"),
        P("tp", "sp", None),
    )
    out_specs = (
        P(None, "tp", None, "sp"),
        P(None, "tp", "sp"),
        P(None, "tp"),
        P(None, ("sp", "tp")),
    )
    return jax.shard_map(body, mesh=mesh, in_specs=in_specs, out_specs=out_specs, check_vma=False)
```

```python
import jax
import jax.numpy as jnp
from jax import lax
from jax.experimental import pallas as pl
from jax.experimental.pallas import tpu as pltpu
from jax.sharding import PartitionSpec as P

MESH_ID = pl.DeviceIdType.MESH
F32 = jnp.float32
BF16 = jnp.bfloat16
NT = (((1,), (1,)), ((), ()))
KEY0 = 16
VAL0 = 144
CHUNKS = 4


def log_sigmoid(x):
    return jnp.minimum(x, 0.0) - jnp.log1p(jnp.exp(-jnp.abs(x)))


def three_parts(x):
    high = x.astype(BF16)
    rest = x - high.astype(F32)
    middle = rest.astype(BF16)
    low = (rest - middle.astype(F32)).astype(BF16)
    return high, middle, low


def kernel(
    prompt, key_w, value_w, in_w, fg_w, fg_bias, taps, extra, query, new_key, new_value,
    new_in, new_fg, out_w,
    packed,
    p_buf, wk_buf, wv_buf, wt_buf, hp_buf, r_buf, tri_buf, par_buf, mem_buf, e_buf,
    h_send, h_recv, e_recv, m_recv, ow_recv, part_buf, part_recv, f_buf, f_recv, lhs_buf, key_buf,
    along_buf, suf_buf, ow_buf, col_buf,
    in_v, fg_v, bias_v, taps_v, extra_v, query_v, key_v, value_v, nin_v, nfg_v,
    w_sem, p_sem, hp_sem, small_sem, ow_local, h_ssem, h_rsem, e_ssem, e_rsem, m_ssem, m_rsem,
    ow_ssem, ow_rsem, o_ssem, o_rsem, f_ssem, f_rsem,
):
    seqs, length, width = p_buf.shape
    sp_n, tp_n = lax.axis_size("sp"), lax.axis_size("tp")
    sp, tp = lax.axis_index("sp"), lax.axis_index("tp")
    step = width // CHUNKS

    barrier = pltpu.get_barrier_semaphore()

    def sp_peer(d):
        return lax.rem(sp + d, sp_n)

    def tp_peer(d):
        return lax.rem(tp + d, tp_n)

    small_pairs = (
        (in_w, in_v), (fg_w, fg_v), (fg_bias, bias_v), (taps, taps_v), (extra, extra_v),
        (query, query_v), (new_key, key_v), (new_value, value_v), (new_in, nin_v),
        (new_fg, nfg_v),
    )
    small_copies = [
        pltpu.make_async_copy(src, dst, small_sem.at[i])
        for i, (src, dst) in enumerate(small_pairs)
    ]
    hp_copies = []
    for s in range(seqs):
        for side, row in ((0, 0), (1, length - 8)):
            g = 2 * s + side
            hp_copies.append(
                pltpu.make_async_copy(
                    prompt.at[s, pl.ds(row, 8), :], hp_buf.at[pl.ds(8 * g, 8), :], hp_sem.at[g]
                )
            )
    wk_copies = [
        pltpu.make_async_copy(key_w.at[rows, :], wk_buf.at[rows, :], w_sem.at[0, i])
        for i, rows in enumerate((pl.ds(0, width // 2), pl.ds(width // 2, width // 2)))
    ]
    w_copies, p_copies = [], []
    for c in range(CHUNKS):
        rows = pl.ds(c * step, step)
        w_copies.append(
            pltpu.make_async_copy(value_w.at[rows, :], wv_buf.at[rows, :], w_sem.at[1, c])
        )
        p_copies.append(
            pltpu.make_async_copy(prompt.at[0, :, rows], p_buf.at[0, :, rows], p_sem.at[0, c])
        )
    s_copies = [p_copies]
    for s in range(1, seqs):
        group = []
        for c in range(CHUNKS):
            cols = pl.ds(c * step, step)
            group.append(
                pltpu.make_async_copy(prompt.at[s, :, cols], p_buf.at[s, :, cols], p_sem.at[s, c])
            )
        s_copies.append(group)

    def start(copies):
        for copy in copies:
            copy.start()

    def finished(copies):
        for copy in copies:
            copy.wait()

    start(wk_copies)
    start(hp_copies)
    start(w_copies[:1])
    start(p_copies[:1])
    start(small_copies)
    start(w_copies[1:2])
    start(p_copies[1:2])
    start(w_copies[2:3])
    start(p_copies[2:3])

    @pl.loop(1, sp_n)
    def _(d):
        pl.semaphore_signal(barrier, inc=1, device_id=(sp_peer(d), tp), device_id_type=MESH_ID)

    @pl.loop(1, tp_n)
    def _(d):
        pl.semaphore_signal(barrier, inc=1, device_id=(sp, tp_peer(d)), device_id_type=MESH_ID)

    tri_buf[...] = (
        lax.broadcasted_iota(jnp.int32, (length, length), 0)
        > lax.broadcasted_iota(jnp.int32, (length, length), 1)
    ).astype(F32).astype(BF16)

    lane = lax.broadcasted_iota(jnp.int32, (1, 128), 1)
    first_head = lane < 64

    def halves(left, right):
        return jnp.where(first_head, left, right)

    def chunk_of(c):
        return pl.ds(c * step, step)

    def turn(c):
        cols = chunk_of(c)
        wt_buf[KEY0:VAL0, cols] = jnp.transpose(wk_buf[cols, :])
        wt_buf[VAL0:, cols] = jnp.transpose(wv_buf[cols, :])

    def chunk_dot(s, c):
        cols = chunk_of(c)
        part = lax.dot_general(
            wt_buf[:, cols], p_buf[s, :, cols], NT, preferred_element_type=F32
        )
        if c == 0:
            r_buf[s] = part
        else:
            r_buf[s] = r_buf[s] + part

    finished(wk_copies)
    finished(hp_copies)
    finished(small_copies)
    finished(w_copies[:1])
    start(w_copies[3:])
    start(p_copies[3:])
    start(s_copies[1][:2])
    edge = jnp.dot(hp_buf[...], wk_buf[...], preferred_element_type=F32).astype(BF16).astype(F32)
    zero4 = jnp.zeros((4, 128), F32)
    h_send[0] = jnp.concatenate(
        [edge[16 * s + 15 : 16 * s + 16] for s in range(seqs)] + [zero4], axis=0
    )
    h_send[1] = jnp.concatenate(
        [edge[16 * s : 16 * s + 1] for s in range(seqs)] + [zero4], axis=0
    )

    gate_rows = jnp.concatenate(
        [
            in_v[...].astype(F32), jnp.zeros((6, width), F32),
            fg_v[...].astype(F32), jnp.zeros((6, width), F32),
        ],
        axis=0,
    )
    wt_buf[0:KEY0, :] = gate_rows.astype(BF16)
    turn(0)

    finished(p_copies[:1])
    finished(w_copies[1:2])
    start(s_copies[1][2:])
    chunk_dot(0, 0)
    turn(1)
    pl.semaphore_wait(barrier, sp_n - 1 + tp_n - 1)
    halo_copies = []
    for side, d in ((0, 1), (1, sp_n - 1)):
        copy = pltpu.make_async_remote_copy(
            src_ref=h_send.at[side],
            dst_ref=h_recv.at[side],
            send_sem=h_ssem.at[side],
            recv_sem=h_rsem.at[side],
            device_id=(sp_peer(d), tp),
            device_id_type=MESH_ID,
        )
        copy.start()
        halo_copies.append(copy)

    finished(p_copies[1:3])
    finished(w_copies[2:])
    start(s_copies[2])
    turn(2)
    chunk_dot(0, 1)
    turn(3)
    chunk_dot(0, 2)

    for s in range(seqs):
        rows = pl.ds(s, 1)
        par_buf[0, rows, :] = jnp.concatenate(
            [query_v[s, 0:1, :].astype(F32), query_v[s, 1:2, :].astype(F32)], axis=1
        )
        par_buf[1, rows, :] = jnp.concatenate(
            [key_v[s, 0:1, :].astype(F32), key_v[s, 1:2, :].astype(F32)], axis=1
        )
        par_buf[2, rows, :] = halves(nin_v[0:1, s : s + 1], nin_v[1:2, s : s + 1])
        par_buf[3, rows, :] = halves(nfg_v[0:1, s : s + 1], nfg_v[1:2, s : s + 1])
        fresh = value_v[s].astype(F32)
        spread = jnp.concatenate([fresh, jnp.zeros((2, 120), F32)], axis=1)
        left = pltpu.roll(spread, 8 * lax.rem(sp, 8), 1)
        fresh_row = halves(left[0:1], pltpu.roll(left[1:2], 64, 1))
        f_buf[s : s + 1, :] = jnp.where(sp < 8, fresh_row, 0.0)
        f_buf[4 + s : 5 + s, :] = jnp.where(sp < 8, 0.0, fresh_row)
    col_buf[:, 0:8] = jnp.transpose(
        jnp.concatenate(
            [taps_v[...].astype(F32), jnp.zeros((1, 128), F32), par_buf[0, 0:4, :]], axis=0
        )
    )

    bias_col = jnp.where(
        lax.broadcasted_iota(jnp.int32, (2, 1), 0) == 0, bias_v[0], bias_v[1]
    )

    cols_of = out_w.shape[2] // sp_n

    def ow_slot(ref):
        return ref.at[sp // 8, :, lax.rem(sp, 8)]

    def ow_cols(j):
        return out_w.at[:, :, pl.ds(pl.multiple_of(j * cols_of, cols_of), cols_of)]

    pos = lax.broadcasted_iota(jnp.int32, (1, length), 1)
    my_rows = pl.multiple_of(8 * sp, 8)
    my_tile = pl.multiple_of(8 * sp, 8)

    def slot_rows(s, size):
        return pl.ds(pl.multiple_of((s * sp_n + sp) * size, size), size)

    def rows_of(x):
        parts = [part.astype(F32) for part in three_parts(x)]
        return jnp.concatenate(parts + [jnp.zeros((10, length), F32)], axis=0).astype(BF16)

    def joined(x, h):
        return x[h : h + 1] + x[2 + h : 3 + h] + x[4 + h : 5 + h]

    def suffix(s):
        fg_pre = r_buf[s, 8:10, :].astype(BF16).astype(F32)
        log_f = log_sigmoid(fg_pre + bias_col) + extra_v[s]
        if s == seqs - 1:
            sums = jnp.dot(rows_of(log_f), tri_buf[...], preferred_element_type=F32)
            later = sums[0:2] + sums[2:4] + sums[4:6]
        else:
            later = jnp.where(pos < length - 1, pltpu.roll(log_f, length - 1, 1), 0.0)
            shift = 1
            while shift < length:
                later = later + jnp.where(
                    pos < length - shift, pltpu.roll(later, length - shift, 1), 0.0
                )
                shift *= 2
        suf_buf[s, 0:2, :] = later
        suf_buf[s, 2:4, :] = jnp.broadcast_to(later[:, 0:1] + log_f[:, 0:1], (2, length))

    def keys(s):
        key = r_buf[s, KEY0:VAL0, :].astype(BF16).astype(F32)
        earlier = jnp.where(pos == 0, col_buf[:, 8 + s : 9 + s], pltpu.roll(key, 1, 1))
        coming = jnp.where(
            pos == length - 1, col_buf[:, 16 + s : 17 + s], pltpu.roll(key, length - 1, 1)
        )
        mixed = col_buf[:, 0:1] * earlier + col_buf[:, 1:2] * key + col_buf[:, 2:3] * coming
        key_rows = (mixed * jax.nn.sigmoid(mixed) * 0.125).astype(BF16)
        key_buf[s] = key_rows
        prod = key_rows.astype(F32) * col_buf[:, 4 + s : 5 + s]
        along = jnp.concatenate(
            [
                jnp.sum(prod[0:64], axis=0, keepdims=True),
                jnp.sum(prod[64:128], axis=0, keepdims=True),
            ],
            axis=0,
        )
        along_buf[s] = rows_of(along)

    def weigh(s):
        in_pre = r_buf[s, 0:2, :].astype(BF16).astype(F32)
        gate = in_pre + suf_buf[s, 0:2, :]
        top = jnp.max(gate, axis=1, keepdims=True)
        scale = jnp.exp(gate - top)
        lhs_buf[s, 0:16, :] = rows_of(scale)
        for h in range(2):
            value = r_buf[s, VAL0 + 128 * h : VAL0 + 128 * (h + 1), :].astype(BF16).astype(F32)
            lhs_buf[s, 16 + 128 * h : 144 + 128 * h, :] = (value * scale[h : h + 1]).astype(BF16)
        total = suf_buf[s, 2:4, 0:1]
        row = jnp.where(
            lax.rem(lane, 64) < 32,
            halves(total[0:1], total[1:2]),
            halves(top[0:1], top[1:2]),
        )
        e_buf[4 * s + 3 : 4 * s + 4, :] = row

    def outer(s):
        num_parts = lax.dot_general(
            along_buf[s], lhs_buf[s, 16:, :], NT, preferred_element_type=F32
        )
        both = lax.dot_general(lhs_buf[s], key_buf[s], NT, preferred_element_type=F32)
        num0 = joined(num_parts, 0)[:, 0:128]
        num1 = joined(num_parts, 1)[:, 128:256]
        e_buf[4 * s : 4 * s + 1, :] = halves(joined(both, 0), joined(both, 1))
        e_buf[4 * s + 1 : 4 * s + 2, :] = halves(num0, pltpu.roll(num1, 64, 1))
        e_buf[4 * s + 2 : 4 * s + 3, :] = halves(pltpu.roll(num0, 64, 1), num1)
        mem_buf[pl.ds(128 * s, 128), :] = halves(both[16:144], both[144:272])

    z, x = sp // 4, lax.rem(sp, 4)
    offsets = sorted(
        ((dz, dx) for dz in range(4) for dx in range(4) if dz or dx),
        key=lambda o: -(min(o[0], 4 - o[0]) + min(o[1], 4 - o[1])),
    )
    peers = [lax.rem(z + dz, 4) * 4 + lax.rem(x + dx, 4) for dz, dx in offsets]

    def send_sums(s):
        e_recv[slot_rows(s, 4), :] = e_buf[4 * s : 4 * s + 4, :]
        for j in peers:
            pltpu.make_async_remote_copy(
                src_ref=e_buf.at[pl.ds(4 * s, 4), :],
                dst_ref=e_recv.at[slot_rows(s, 4), :],
                send_sem=e_ssem.at[s],
                recv_sem=e_rsem.at[s],
                device_id=(j, tp),
                device_id_type=MESH_ID,
            ).start()

    def send_memory(s):
        m_recv[slot_rows(s, 8), :] = mem_buf[pl.ds(128 * s + my_rows, 8), :]
        for j in peers:
            pltpu.make_async_remote_copy(
                src_ref=mem_buf.at[pl.ds(pl.multiple_of(128 * s + 8 * j, 8), 8), :],
                dst_ref=m_recv.at[slot_rows(s, 8), :],
                send_sem=m_ssem.at[s],
                recv_sem=m_rsem.at[s],
                device_id=(j, tp),
                device_id_type=MESH_ID,
            ).start()

    finished(p_copies[3:])
    finished(s_copies[1][:2])
    start(s_copies[3])
    chunk_dot(0, 3)
    chunk_dot(1, 0)
    chunk_dot(1, 1)
    suffix(0)
    finished(s_copies[1][2:])
    chunk_dot(1, 2)
    chunk_dot(1, 3)

    for copy in halo_copies:
        copy.wait_recv()
    finished(s_copies[2])
    col_buf[:, 8:16] = jnp.where(sp == 0, 0.0, jnp.transpose(h_recv[0]))
    col_buf[:, 16:24] = jnp.where(sp == sp_n - 1, 0.0, jnp.transpose(h_recv[1]))
    chunk_dot(2, 0)
    own_ow = pltpu.make_async_copy(ow_cols(sp), ow_slot(ow_recv), ow_local)
    own_ow.start()
    f_recv[pl.ds(my_tile, 8), :] = f_buf[...]
    for j in peers:
        pltpu.make_async_remote_copy(
            src_ref=f_buf,
            dst_ref=f_recv.at[pl.ds(my_tile, 8), :],
            send_sem=f_ssem,
            recv_sem=f_rsem,
            device_id=(j, tp),
            device_id_type=MESH_ID,
        ).start()
        pltpu.make_async_remote_copy(
            src_ref=ow_cols(j),
            dst_ref=ow_slot(ow_recv),
            send_sem=ow_ssem,
            recv_sem=ow_rsem,
            device_id=(j, tp),
            device_id_type=MESH_ID,
        ).start()

    chunk_dot(2, 1)
    keys(0)
    weigh(0)
    chunk_dot(2, 2)
    suffix(1)
    chunk_dot(2, 3)

    finished(s_copies[3])
    outer(0)
    chunk_dot(3, 0)
    keys(1)
    weigh(1)
    send_sums(0)
    send_memory(0)
    chunk_dot(3, 1)
    suffix(2)
    outer(1)
    chunk_dot(3, 2)
    keys(2)
    weigh(2)
    send_sums(1)
    chunk_dot(3, 3)
    outer(2)
    suffix(3)
    send_sums(2)
    keys(3)
    weigh(3)
    outer(3)
    send_sums(3)
    send_memory(1)
    send_memory(2)
    send_memory(3)

    def take(ref, sem, count):
        view = ref.at[pl.ds(0, count), :]
        pltpu.make_async_copy(view, view, sem).wait()

    own_ow.wait()
    ow_bytes = out_w.at[:, :, pl.ds(0, cols_of * (sp_n - 1))]
    pltpu.make_async_copy(ow_bytes, ow_bytes, ow_rsem).wait()
    ow_buf[...] = ow_recv[...].reshape(256, cols_of)
    take(f_recv, f_rsem, 8 * (sp_n - 1))
    fresh_sum = f_recv[0:8, :]
    for i in range(1, sp_n):
        fresh_sum = fresh_sum + f_recv[8 * i : 8 * i + 8, :]

    row16 = lax.broadcasted_iota(jnp.int32, (sp_n, 128), 0)
    low_lanes = lax.rem(lax.broadcasted_iota(jnp.int32, (sp_n, 128), 1), 64) < 32

    def by_head(x):
        left = jnp.sum(jnp.where(first_head, x, 0.0), axis=1, keepdims=True)
        right = jnp.sum(jnp.where(first_head, 0.0, x), axis=1, keepdims=True)
        return halves(left, right)

    def combine(s):
        def rows_at(k):
            return e_recv[pl.ds(s * sp_n * 4 + k, sp_n, stride=4), :]

        stats = rows_at(3)
        totals = jnp.where(low_lanes, stats, pltpu.roll(stats, 32, 1))
        tops = jnp.where(low_lanes, pltpu.roll(stats, 96, 1), stats)
        later = jnp.where(row16 < sp_n - 1, pltpu.roll(totals, sp_n - 1, 0), 0.0)
        shift = 1
        while shift < sp_n:
            later = later + jnp.where(
                row16 < sp_n - shift, pltpu.roll(later, sp_n - shift, 0), 0.0
            )
            shift *= 2
        gate = tops + later
        peak = jnp.max(gate, axis=0, keepdims=True)
        factor = jnp.exp(gate - peak)

        def summed(k):
            return jnp.sum(factor * rows_at(k), axis=0, keepdims=True)

        norm, num_a, num_b = summed(0), summed(1), summed(2)
        q, k = par_buf[0, s : s + 1, :], par_buf[1, s : s + 1, :]
        gate_in, gate_fg = par_buf[2, s : s + 1, :], par_buf[3, s : s + 1, :]
        kept = log_sigmoid(gate_fg) + peak
        new_peak = jnp.maximum(kept, gate_in)
        old_scale = jnp.exp(kept - new_peak)
        new_scale = jnp.exp(gate_in - new_peak)
        denom = jnp.maximum(jnp.abs(by_head(q * (old_scale * norm + new_scale * k))), 1.0)
        fresh_scale = new_scale * by_head(q * k)
        read_a = (old_scale * num_a + fresh_scale * fresh_sum[s : s + 1]) / denom
        read_b = (old_scale * num_b + fresh_scale * fresh_sum[4 + s : 5 + s]) / denom
        packed[32 + s : 33 + s, :] = pltpu.roll(norm, lax.rem(128 - 4 * sp, 128), 1)
        packed[36 + s : 37 + s, :] = peak
        return jnp.concatenate([read_a, read_b], axis=1), factor

    reads, factors = [], []
    for s in range(seqs - 1):
        take(e_recv, e_rsem.at[s], 4 * (sp_n - 1))
        row, factor = combine(s)
        reads.append(row)
        factors.append(factor)
    take(e_recv, e_rsem.at[seqs - 1], 4 * (sp_n - 1))
    row, factor = combine(seqs - 1)
    reads.append(row)
    factors.append(factor)

    read = jnp.concatenate(reads + [jnp.zeros((12, 256), F32)], axis=0).astype(BF16)
    part = jnp.dot(read, ow_buf[...], preferred_element_type=F32)[0:4]
    part_buf[0] = part[:, 0:128]
    part_buf[1] = part[:, 128:256]
    part_recv[tp] = part_buf[tp // 4]
    y, core = tp // 2, lax.rem(tp, 2)
    for dy, dc in ((2, 1), (2, 0), (1, 1), (3, 1), (1, 0), (3, 0), (0, 1)):
        j = lax.rem(y + dy, 4) * 2 + lax.rem(core + dc, 2)
        pltpu.make_async_remote_copy(
            src_ref=part_buf.at[j // 4],
            dst_ref=part_recv.at[tp],
            send_sem=o_ssem,
            recv_sem=o_rsem,
            device_id=(sp, j),
            device_id_type=MESH_ID,
        ).start()

    for s in range(seqs):
        take(m_recv, m_rsem.at[s], 8 * (sp_n - 1))
    for s in range(seqs):
        memory = jnp.zeros((8, 128), F32)
        for i in range(sp_n):
            base = (s * sp_n + i) * 8
            memory = memory + factors[s][i : i + 1] * m_recv[base : base + 8, :]
        packed[8 * s : 8 * s + 8, :] = memory

    view = part_recv.at[pl.ds(0, tp_n - 1)]
    pltpu.make_async_copy(view, view, o_rsem).wait()
    whole = part_recv[0]
    for i in range(1, tp_n):
        whole = whole + part_recv[i]
    packed[40:44, :] = pltpu.roll(whole, lax.rem(128 - 32 * lax.rem(tp, 4), 128), 1)

    for copy in halo_copies:
        copy.wait_send()
    pltpu.make_async_copy(ow_bytes, ow_bytes, ow_ssem).wait()
    take(f_recv, f_ssem, 8 * (sp_n - 1))
    for s in range(seqs):
        take(e_recv, e_ssem.at[s], 4 * (sp_n - 1))
        take(m_recv, m_ssem.at[s], 8 * (sp_n - 1))
    pltpu.make_async_copy(view, view, o_ssem).wait()


def unpack(packed, mem_out, norm_out, peak_out, read_out):
    seqs = mem_out.shape[0]
    for s in range(seqs):
        rows = packed[8 * s : 8 * s + 8, :]
        mem_out[s, 0] = rows[:, 0:64].astype(BF16)
        mem_out[s, 1] = rows[:, 64:128].astype(BF16)
        norm = packed[32 + s : 33 + s, :]
        norm_out[s, 0:1, :] = norm[:, 0:4].astype(BF16)
        norm_out[s, 1:2, :] = norm[:, 64:68].astype(BF16)
        peak = packed[36 + s : 37 + s, :]
        peak_out[0:1, s : s + 1] = peak[:, 0:1]
        peak_out[1:2, s : s + 1] = peak[:, 64:65]
    read_out[...] = packed[40:44, 0:32].astype(BF16)


def body(
    prompt, key_weight, value_weight, input_gate_weight, forget_gate_weight, forget_bias,
    key_taps, extra_decay, new_query, new_key, new_value, new_input_gate, new_forget_gate,
    out_weight,
):
    seqs, length, width = prompt.shape
    sp_n = lax.axis_size("sp")
    tp_n = lax.axis_size("tp")
    cols_of = out_weight.shape[2] // sp_n
    any_spec = pl.BlockSpec(memory_space=pl.ANY)
    vmem = pl.BlockSpec(memory_space=pltpu.VMEM)
    dma = pltpu.SemaphoreType.DMA
    packed = pl.pallas_call(
        kernel,
        out_shape=pltpu.VMEM((48, 128), F32),
        in_specs=[any_spec] * 14,
        out_specs=vmem,
        scratch_shapes=[
            pltpu.VMEM((seqs, length, width), BF16),
            pltpu.VMEM((width, 128), BF16),
            pltpu.VMEM((width, 256), BF16),
            pltpu.VMEM((400, width), BF16),
            pltpu.VMEM((64, width), BF16),
            pltpu.VMEM((seqs, 400, length), F32),
            pltpu.VMEM((length, length), BF16),
            pltpu.VMEM((4, 8, 128), F32),
            pltpu.VMEM((seqs * 128, 128), F32),
            pltpu.VMEM((seqs * 4, 128), F32),
            pltpu.VMEM((2, 8, 128), F32),
            pltpu.VMEM((2, 8, 128), F32),
            pltpu.VMEM((seqs * sp_n * 4, 128), F32),
            pltpu.VMEM((seqs * sp_n * 8, 128), F32),
            pltpu.VMEM((2, 2, 8, 8, cols_of), BF16),
            pltpu.VMEM((2, 4, 128), F32),
            pltpu.VMEM((tp_n, 4, 128), F32),
            pltpu.VMEM((8, 128), F32),
            pltpu.VMEM((sp_n * 8, 128), F32),
            pltpu.VMEM((seqs, 272, length), BF16),
            pltpu.VMEM((seqs, 128, length), BF16),
            pltpu.VMEM((seqs, 16, length), BF16),
            pltpu.VMEM((seqs, 4, length), F32),
            pltpu.VMEM((256, cols_of), BF16),
            pltpu.VMEM((128, 128), F32),
            pltpu.VMEM((2, width), BF16),
            pltpu.VMEM((2, width), BF16),
            pltpu.SMEM((2,), F32),
            pltpu.VMEM((3, 128), BF16),
            pltpu.VMEM((seqs, 2, length), F32),
            pltpu.VMEM((seqs, 2, 64), BF16),
            pltpu.VMEM((seqs, 2, 64), BF16),
            pltpu.VMEM((seqs, 2, 8), BF16),
            pltpu.VMEM((2, seqs), F32),
            pltpu.VMEM((2, seqs), F32),
            dma((2, CHUNKS)),
            dma((seqs, CHUNKS)),
            dma((2 * seqs,)),
            dma((10,)),
            dma,
            dma((2,)),
            dma((2,)),
            dma((seqs,)),
            dma((seqs,)),
            dma((seqs,)),
            dma((seqs,)),
            dma,
            dma,
            dma,
            dma,
            dma,
            dma,
        ],
        compiler_params=pltpu.CompilerParams(
            collective_id=0, has_side_effects=True, vmem_limit_bytes=60 * 1024 * 1024
        ),
        name="prompt_state",
    )(
        prompt,
        key_weight,
        value_weight,
        input_gate_weight.T,
        forget_gate_weight.T,
        forget_bias,
        key_taps,
        jnp.transpose(extra_decay, (0, 2, 1)),
        new_query,
        new_key,
        new_value,
        new_input_gate.T,
        new_forget_gate.T,
        out_weight,
    )
    memory, norm, peak, read = pl.pallas_call(
        unpack,
        out_shape=(
            jax.ShapeDtypeStruct((seqs, 2, 8, 64), BF16),
            jax.ShapeDtypeStruct((seqs, 2, 4), BF16),
            jax.ShapeDtypeStruct((2, seqs), F32),
            jax.ShapeDtypeStruct((seqs, 32), BF16),
        ),
        in_specs=[vmem],
        out_specs=(vmem,) * 4,
        compiler_params=pltpu.CompilerParams(vmem_limit_bytes=1024 * 1024),
        name="unpack",
    )(packed)
    return jnp.transpose(memory, (0, 1, 3, 2)), norm, peak.T, read


def solution(mesh):
    in_specs = (
        P(None, "sp", None),
        P(None, "tp"),
        P(None, "tp"),
        P(None, "tp"),
        P(None, "tp"),
        P("tp"),
        P(None, "tp"),
        P(None, "sp", "tp"),
        P(None, "tp", None),
        P(None, "tp", None),
        P(None, "tp", "sp"),
        P(None, "tp"),
        P(None, "tp"),
        P("tp", "sp", None),
    )
    out_specs = (
        P(None, "tp", None, "sp"),
        P(None, "tp", "sp"),
        P(None, "tp"),
        P(None, ("sp", "tp")),
    )
    return jax.shard_map(body, mesh=mesh, in_specs=in_specs, out_specs=out_specs, check_vma=False)
```

```python
import jax
import jax.numpy as jnp
from jax import lax
from jax.experimental import pallas as pl
from jax.experimental.pallas import tpu as pltpu
from jax.sharding import PartitionSpec as P

MESH_ID = pl.DeviceIdType.MESH
F32 = jnp.float32
BF16 = jnp.bfloat16
NT = (((1,), (1,)), ((), ()))
KEY0 = 16
VAL0 = 144
CHUNKS = 4


def log_sigmoid(x):
    return jnp.minimum(x, 0.0) - jnp.log1p(jnp.exp(-jnp.abs(x)))


def three_parts(x):
    high = x.astype(BF16)
    rest = x - high.astype(F32)
    middle = rest.astype(BF16)
    low = (rest - middle.astype(F32)).astype(BF16)
    return high, middle, low


def kernel(
    prompt, key_w, value_w, in_w, fg_w, fg_bias, taps, extra, query, new_key, new_value,
    new_in, new_fg, out_w,
    packed,
    p_buf, wk_buf, wv_buf, wt_buf, hp_buf, r_buf, tri_buf, par_buf, mem_buf, e_buf,
    h_send, h_recv, e_recv, m_recv, ow_recv, part_buf, part_recv, f_buf, f_recv, lhs_buf, key_buf,
    along_buf, suf_buf, ow_buf, col_buf,
    in_v, fg_v, bias_v, taps_v, extra_v, query_v, key_v, value_v, nin_v, nfg_v,
    w_sem, p_sem, hp_sem, small_sem, ow_local, h_ssem, h_rsem, e_ssem, e_rsem, m_ssem, m_rsem,
    ow_ssem, ow_rsem, o_ssem, o_rsem, f_ssem, f_rsem,
):
    seqs, length, width = p_buf.shape
    sp_n, tp_n = lax.axis_size("sp"), lax.axis_size("tp")
    sp, tp = lax.axis_index("sp"), lax.axis_index("tp")
    step = width // CHUNKS

    barrier = pltpu.get_barrier_semaphore()

    def sp_peer(d):
        return lax.rem(sp + d, sp_n)

    def tp_peer(d):
        return lax.rem(tp + d, tp_n)

    small_pairs = (
        (in_w, in_v), (fg_w, fg_v), (fg_bias, bias_v), (taps, taps_v), (extra, extra_v),
        (query, query_v), (new_key, key_v), (new_value, value_v), (new_in, nin_v),
        (new_fg, nfg_v),
    )
    small_copies = [
        pltpu.make_async_copy(src, dst, small_sem.at[i])
        for i, (src, dst) in enumerate(small_pairs)
    ]
    hp_copies = []
    for s in range(seqs):
        for side, row in ((0, 0), (1, length - 8)):
            g = 2 * s + side
            hp_copies.append(
                pltpu.make_async_copy(
                    prompt.at[s, pl.ds(row, 8), :], hp_buf.at[pl.ds(8 * g, 8), :], hp_sem
                )
            )
    wk_copies = [
        pltpu.make_async_copy(key_w.at[rows, :], wk_buf.at[rows, :], w_sem.at[0])
        for rows in (pl.ds(0, width // 2), pl.ds(width // 2, width // 2))
    ]
    w_copies, p_copies = [], []
    for c in range(CHUNKS):
        rows = pl.ds(c * step, step)
        w_copies.append(
            pltpu.make_async_copy(value_w.at[rows, :], wv_buf.at[rows, :], w_sem.at[1 + c])
        )
        p_copies.append(
            pltpu.make_async_copy(prompt.at[0, :, rows], p_buf.at[0, :, rows], p_sem.at[c])
        )
    s_copies = [p_copies]
    for s in range(1, seqs):
        group = []
        for c in range(CHUNKS):
            cols = pl.ds(c * step, step)
            s_sem = p_sem.at[CHUNKS + c // 2 if s == 1 else CHUNKS + s]
            group.append(
                pltpu.make_async_copy(prompt.at[s, :, cols], p_buf.at[s, :, cols], s_sem)
            )
        s_copies.append(group)

    def start(copies):
        for copy in copies:
            copy.start()

    def finished(copies):
        for copy in copies:
            copy.wait()

    def landed(view, sem):
        pltpu.make_async_copy(view, view, sem).wait()

    start(wk_copies)
    start(hp_copies)
    start(w_copies[:1])
    start(p_copies[:1])
    start(small_copies)
    start(w_copies[1:2])
    start(p_copies[1:2])
    start(w_copies[2:3])
    start(p_copies[2:3])

    @pl.loop(1, sp_n)
    def _(d):
        pl.semaphore_signal(barrier, inc=1, device_id=(sp_peer(d), tp), device_id_type=MESH_ID)

    @pl.loop(1, tp_n)
    def _(d):
        pl.semaphore_signal(barrier, inc=1, device_id=(sp, tp_peer(d)), device_id_type=MESH_ID)

    tri_buf[...] = (
        lax.broadcasted_iota(jnp.int32, (length, length), 0)
        > lax.broadcasted_iota(jnp.int32, (length, length), 1)
    ).astype(F32).astype(BF16)

    lane = lax.broadcasted_iota(jnp.int32, (1, 128), 1)
    first_head = lane < 64

    def halves(left, right):
        return jnp.where(first_head, left, right)

    def chunk_of(c):
        return pl.ds(c * step, step)

    def turn(c):
        cols = chunk_of(c)
        wt_buf[KEY0:VAL0, cols] = jnp.transpose(wk_buf[cols, :])
        wt_buf[VAL0:, cols] = jnp.transpose(wv_buf[cols, :])

    def chunk_dot(s, c):
        cols = chunk_of(c)
        part = lax.dot_general(
            wt_buf[:, cols], p_buf[s, :, cols], NT, preferred_element_type=F32
        )
        if c == 0:
            r_buf[s] = part
        else:
            r_buf[s] = r_buf[s] + part

    landed(wk_buf, w_sem.at[0])
    landed(hp_buf, hp_sem)
    finished(small_copies)
    finished(w_copies[:1])
    start(w_copies[3:])
    start(p_copies[3:])
    start(s_copies[1][:2])
    edge = jnp.dot(hp_buf[...], wk_buf[...], preferred_element_type=F32).astype(BF16).astype(F32)
    zero4 = jnp.zeros((4, 128), F32)
    h_send[0] = jnp.concatenate(
        [edge[16 * s + 15 : 16 * s + 16] for s in range(seqs)] + [zero4], axis=0
    )
    h_send[1] = jnp.concatenate(
        [edge[16 * s : 16 * s + 1] for s in range(seqs)] + [zero4], axis=0
    )

    gate_rows = jnp.concatenate(
        [
            in_v[...].astype(F32), jnp.zeros((6, width), F32),
            fg_v[...].astype(F32), jnp.zeros((6, width), F32),
        ],
        axis=0,
    )
    wt_buf[0:KEY0, :] = gate_rows.astype(BF16)
    turn(0)

    finished(p_copies[:1])
    finished(w_copies[1:2])
    start(s_copies[1][2:])
    chunk_dot(0, 0)
    turn(1)
    pl.semaphore_wait(barrier, sp_n - 1 + tp_n - 1)
    for side, d in ((0, 1), (1, sp_n - 1)):
        copy = pltpu.make_async_remote_copy(
            src_ref=h_send.at[side],
            dst_ref=h_recv.at[side],
            send_sem=h_ssem,
            recv_sem=h_rsem,
            device_id=(sp_peer(d), tp),
            device_id_type=MESH_ID,
        )
        copy.start()

    finished(p_copies[1:2])
    finished(w_copies[2:3])
    chunk_dot(0, 1)
    turn(2)
    finished(p_copies[2:3])
    finished(w_copies[3:])
    start(s_copies[2])
    chunk_dot(0, 2)
    turn(3)

    for s in range(seqs):
        rows = pl.ds(s, 1)
        par_buf[0, rows, :] = jnp.concatenate(
            [query_v[s, 0:1, :].astype(F32), query_v[s, 1:2, :].astype(F32)], axis=1
        )
        par_buf[1, rows, :] = jnp.concatenate(
            [key_v[s, 0:1, :].astype(F32), key_v[s, 1:2, :].astype(F32)], axis=1
        )
        par_buf[2, rows, :] = halves(nin_v[0:1, s : s + 1], nin_v[1:2, s : s + 1])
        par_buf[3, rows, :] = halves(nfg_v[0:1, s : s + 1], nfg_v[1:2, s : s + 1])
        fresh = value_v[s].astype(F32)
        spread = jnp.concatenate([fresh, jnp.zeros((2, 120), F32)], axis=1)
        left = pltpu.roll(spread, 8 * lax.rem(sp, 8), 1)
        fresh_row = halves(left[0:1], pltpu.roll(left[1:2], 64, 1))
        f_buf[s : s + 1, :] = jnp.where(sp < 8, fresh_row, 0.0)
        f_buf[4 + s : 5 + s, :] = jnp.where(sp < 8, 0.0, fresh_row)
    col_buf[:, 0:8] = jnp.transpose(
        jnp.concatenate(
            [taps_v[...].astype(F32), jnp.zeros((1, 128), F32), par_buf[0, 0:4, :]], axis=0
        )
    )

    bias_col = jnp.where(
        lax.broadcasted_iota(jnp.int32, (2, 1), 0) == 0, bias_v[0], bias_v[1]
    )

    cols_of = out_w.shape[2] // sp_n

    def ow_slot(ref):
        return ref.at[sp // 8, :, lax.rem(sp, 8)]

    def ow_cols(j):
        return out_w.at[:, :, pl.ds(pl.multiple_of(j * cols_of, cols_of), cols_of)]

    pos = lax.broadcasted_iota(jnp.int32, (1, length), 1)
    my_rows = pl.multiple_of(8 * sp, 8)
    my_tile = pl.multiple_of(8 * sp, 8)

    def slot_rows(s, size):
        return pl.ds(pl.multiple_of((s * sp_n + sp) * size, size), size)

    def rows_of(x):
        parts = [part.astype(F32) for part in three_parts(x)]
        return jnp.concatenate(parts + [jnp.zeros((10, length), F32)], axis=0).astype(BF16)

    def joined(x, h):
        return x[h : h + 1] + x[2 + h : 3 + h] + x[4 + h : 5 + h]

    def suffix(s):
        fg_pre = r_buf[s, 8:10, :].astype(BF16).astype(F32)
        log_f = log_sigmoid(fg_pre + bias_col) + extra_v[s]
        if s == seqs - 1:
            sums = jnp.dot(rows_of(log_f), tri_buf[...], preferred_element_type=F32)
            later = sums[0:2] + sums[2:4] + sums[4:6]
        else:
            later = jnp.where(pos < length - 1, pltpu.roll(log_f, length - 1, 1), 0.0)
            shift = 1
            while shift < length:
                later = later + jnp.where(
                    pos < length - shift, pltpu.roll(later, length - shift, 1), 0.0
                )
                shift *= 2
        suf_buf[s, 0:2, :] = later
        suf_buf[s, 2:4, :] = jnp.broadcast_to(later[:, 0:1] + log_f[:, 0:1], (2, length))

    def keys(s):
        key = r_buf[s, KEY0:VAL0, :].astype(BF16).astype(F32)
        earlier = jnp.where(pos == 0, col_buf[:, 8 + s : 9 + s], pltpu.roll(key, 1, 1))
        coming = jnp.where(
            pos == length - 1, col_buf[:, 16 + s : 17 + s], pltpu.roll(key, length - 1, 1)
        )
        mixed = col_buf[:, 0:1] * earlier + col_buf[:, 1:2] * key + col_buf[:, 2:3] * coming
        key_rows = (mixed * jax.nn.sigmoid(mixed) * 0.125).astype(BF16)
        key_buf[s] = key_rows
        prod = key_rows.astype(F32) * col_buf[:, 4 + s : 5 + s]
        along = jnp.concatenate(
            [
                jnp.sum(prod[0:64], axis=0, keepdims=True),
                jnp.sum(prod[64:128], axis=0, keepdims=True),
            ],
            axis=0,
        )
        along_buf[s] = rows_of(along)

    def weigh(s):
        in_pre = r_buf[s, 0:2, :].astype(BF16).astype(F32)
        gate = in_pre + suf_buf[s, 0:2, :]
        top = jnp.max(gate, axis=1, keepdims=True)
        scale = jnp.exp(gate - top)
        lhs_buf[s, 0:16, :] = rows_of(scale)
        for h in range(2):
            value = r_buf[s, VAL0 + 128 * h : VAL0 + 128 * (h + 1), :].astype(BF16).astype(F32)
            lhs_buf[s, 16 + 128 * h : 144 + 128 * h, :] = (value * scale[h : h + 1]).astype(BF16)
        total = suf_buf[s, 2:4, 0:1]
        row = jnp.where(
            lax.rem(lane, 64) < 32,
            halves(total[0:1], total[1:2]),
            halves(top[0:1], top[1:2]),
        )
        e_buf[4 * s + 3 : 4 * s + 4, :] = row

    def outer(s):
        num_parts = lax.dot_general(
            along_buf[s], lhs_buf[s, 16:, :], NT, preferred_element_type=F32
        )
        both = lax.dot_general(lhs_buf[s], key_buf[s], NT, preferred_element_type=F32)
        num0 = joined(num_parts, 0)[:, 0:128]
        num1 = joined(num_parts, 1)[:, 128:256]
        e_buf[4 * s : 4 * s + 1, :] = halves(joined(both, 0), joined(both, 1))
        e_buf[4 * s + 1 : 4 * s + 2, :] = halves(num0, pltpu.roll(num1, 64, 1))
        e_buf[4 * s + 2 : 4 * s + 3, :] = halves(pltpu.roll(num0, 64, 1), num1)
        mem_buf[pl.ds(128 * s, 128), :] = halves(both[16:144], both[144:272])

    z, x = sp // 4, lax.rem(sp, 4)
    offsets = sorted(
        ((dz, dx) for dz in range(4) for dx in range(4) if dz or dx),
        key=lambda o: -(min(o[0], 4 - o[0]) + min(o[1], 4 - o[1])),
    )
    peers = [lax.rem(z + dz, 4) * 4 + lax.rem(x + dx, 4) for dz, dx in offsets]

    def send_sums(s):
        e_recv[slot_rows(s, 4), :] = e_buf[4 * s : 4 * s + 4, :]
        for j in peers:
            pltpu.make_async_remote_copy(
                src_ref=e_buf.at[pl.ds(4 * s, 4), :],
                dst_ref=e_recv.at[slot_rows(s, 4), :],
                send_sem=e_ssem,
                recv_sem=e_rsem.at[s // (seqs - 1)],
                device_id=(j, tp),
                device_id_type=MESH_ID,
            ).start()

    def send_memory(s):
        m_recv[slot_rows(s, 8), :] = mem_buf[pl.ds(128 * s + my_rows, 8), :]
        for j in peers:
            pltpu.make_async_remote_copy(
                src_ref=mem_buf.at[pl.ds(pl.multiple_of(128 * s + 8 * j, 8), 8), :],
                dst_ref=m_recv.at[slot_rows(s, 8), :],
                send_sem=m_ssem,
                recv_sem=m_rsem,
                device_id=(j, tp),
                device_id_type=MESH_ID,
            ).start()

    finished(p_copies[3:])
    landed(p_buf.at[1, :, pl.ds(0, width // 2)], p_sem.at[CHUNKS])
    start(s_copies[3])
    chunk_dot(0, 3)
    chunk_dot(1, 0)
    chunk_dot(1, 1)
    suffix(0)
    landed(p_buf.at[1, :, pl.ds(width // 2, width // 2)], p_sem.at[CHUNKS + 1])
    chunk_dot(1, 2)
    chunk_dot(1, 3)

    landed(h_recv, h_rsem)
    landed(p_buf.at[2], p_sem.at[CHUNKS + 2])
    col_buf[:, 8:16] = jnp.where(sp == 0, 0.0, jnp.transpose(h_recv[0]))
    col_buf[:, 16:24] = jnp.where(sp == sp_n - 1, 0.0, jnp.transpose(h_recv[1]))
    chunk_dot(2, 0)
    own_ow = pltpu.make_async_copy(ow_cols(sp), ow_slot(ow_recv), ow_local)
    own_ow.start()
    f_recv[pl.ds(my_tile, 8), :] = f_buf[...]
    for j in peers:
        pltpu.make_async_remote_copy(
            src_ref=f_buf,
            dst_ref=f_recv.at[pl.ds(my_tile, 8), :],
            send_sem=f_ssem,
            recv_sem=f_rsem,
            device_id=(j, tp),
            device_id_type=MESH_ID,
        ).start()
        pltpu.make_async_remote_copy(
            src_ref=ow_cols(j),
            dst_ref=ow_slot(ow_recv),
            send_sem=ow_ssem,
            recv_sem=ow_rsem,
            device_id=(j, tp),
            device_id_type=MESH_ID,
        ).start()

    chunk_dot(2, 1)
    keys(0)
    weigh(0)
    chunk_dot(2, 2)
    suffix(1)
    chunk_dot(2, 3)

    landed(p_buf.at[3], p_sem.at[CHUNKS + 3])
    outer(0)
    chunk_dot(3, 0)
    keys(1)
    weigh(1)
    send_sums(0)
    send_memory(0)
    chunk_dot(3, 1)
    suffix(2)
    outer(1)
    chunk_dot(3, 2)
    keys(2)
    weigh(2)
    send_sums(1)
    chunk_dot(3, 3)
    outer(2)
    suffix(3)
    send_sums(2)
    keys(3)
    weigh(3)
    outer(3)
    send_sums(3)
    send_memory(1)
    send_memory(2)
    send_memory(3)

    def take(ref, sem, count):
        view = ref.at[pl.ds(0, count), :]
        pltpu.make_async_copy(view, view, sem).wait()

    own_ow.wait()
    ow_bytes = out_w.at[:, :, pl.ds(0, cols_of * (sp_n - 1))]
    pltpu.make_async_copy(ow_bytes, ow_bytes, ow_rsem).wait()
    ow_buf[...] = ow_recv[...].reshape(256, cols_of)
    take(f_recv, f_rsem, 8 * (sp_n - 1))
    fresh_sum = f_recv[0:8, :]
    for i in range(1, sp_n):
        fresh_sum = fresh_sum + f_recv[8 * i : 8 * i + 8, :]

    row16 = lax.broadcasted_iota(jnp.int32, (sp_n, 128), 0)
    low_lanes = lax.rem(lax.broadcasted_iota(jnp.int32, (sp_n, 128), 1), 64) < 32

    def by_head(x):
        left = jnp.sum(jnp.where(first_head, x, 0.0), axis=1, keepdims=True)
        right = jnp.sum(jnp.where(first_head, 0.0, x), axis=1, keepdims=True)
        return halves(left, right)

    def combine(s):
        def rows_at(k):
            return e_recv[pl.ds(s * sp_n * 4 + k, sp_n, stride=4), :]

        stats = rows_at(3)
        totals = jnp.where(low_lanes, stats, pltpu.roll(stats, 32, 1))
        tops = jnp.where(low_lanes, pltpu.roll(stats, 96, 1), stats)
        later = jnp.where(row16 < sp_n - 1, pltpu.roll(totals, sp_n - 1, 0), 0.0)
        shift = 1
        while shift < sp_n:
            later = later + jnp.where(
                row16 < sp_n - shift, pltpu.roll(later, sp_n - shift, 0), 0.0
            )
            shift *= 2
        gate = tops + later
        peak = jnp.max(gate, axis=0, keepdims=True)
        factor = jnp.exp(gate - peak)

        def summed(k):
            return jnp.sum(factor * rows_at(k), axis=0, keepdims=True)

        norm, num_a, num_b = summed(0), summed(1), summed(2)
        q, k = par_buf[0, s : s + 1, :], par_buf[1, s : s + 1, :]
        gate_in, gate_fg = par_buf[2, s : s + 1, :], par_buf[3, s : s + 1, :]
        kept = log_sigmoid(gate_fg) + peak
        new_peak = jnp.maximum(kept, gate_in)
        old_scale = jnp.exp(kept - new_peak)
        new_scale = jnp.exp(gate_in - new_peak)
        denom = jnp.maximum(jnp.abs(by_head(q * (old_scale * norm + new_scale * k))), 1.0)
        fresh_scale = new_scale * by_head(q * k)
        read_a = (old_scale * num_a + fresh_scale * fresh_sum[s : s + 1]) / denom
        read_b = (old_scale * num_b + fresh_scale * fresh_sum[4 + s : 5 + s]) / denom
        packed[32 + s : 33 + s, :] = pltpu.roll(norm, lax.rem(128 - 4 * sp, 128), 1)
        packed[36 + s : 37 + s, :] = peak
        return jnp.concatenate([read_a, read_b], axis=1), factor

    reads, factors = [], []
    take(e_recv, e_rsem.at[0], 4 * (sp_n - 1) * (seqs - 1))
    for s in range(seqs - 1):
        row, factor = combine(s)
        reads.append(row)
        factors.append(factor)
    take(e_recv, e_rsem.at[1], 4 * (sp_n - 1))
    row, factor = combine(seqs - 1)
    reads.append(row)
    factors.append(factor)

    read = jnp.concatenate(reads + [jnp.zeros((12, 256), F32)], axis=0).astype(BF16)
    part = jnp.dot(read, ow_buf[...], preferred_element_type=F32)[0:4]
    part_buf[0] = part[:, 0:128]
    part_buf[1] = part[:, 128:256]
    part_recv[tp] = part_buf[tp // 4]
    y, core = tp // 2, lax.rem(tp, 2)
    for dy, dc in ((2, 1), (2, 0), (1, 1), (3, 1), (1, 0), (3, 0), (0, 1)):
        j = lax.rem(y + dy, 4) * 2 + lax.rem(core + dc, 2)
        pltpu.make_async_remote_copy(
            src_ref=part_buf.at[j // 4],
            dst_ref=part_recv.at[tp],
            send_sem=o_ssem,
            recv_sem=o_rsem,
            device_id=(sp, j),
            device_id_type=MESH_ID,
        ).start()

    take(m_recv, m_rsem, 8 * (sp_n - 1) * seqs)
    for s in range(seqs):
        memory = jnp.zeros((8, 128), F32)
        for i in range(sp_n):
            base = (s * sp_n + i) * 8
            memory = memory + factors[s][i : i + 1] * m_recv[base : base + 8, :]
        packed[8 * s : 8 * s + 8, :] = memory

    view = part_recv.at[pl.ds(0, tp_n - 1)]
    pltpu.make_async_copy(view, view, o_rsem).wait()
    whole = part_recv[0]
    for i in range(1, tp_n):
        whole = whole + part_recv[i]
    packed[40:44, :] = pltpu.roll(whole, lax.rem(128 - 32 * lax.rem(tp, 4), 128), 1)

    landed(h_recv, h_ssem)
    pltpu.make_async_copy(ow_bytes, ow_bytes, ow_ssem).wait()
    take(f_recv, f_ssem, 8 * (sp_n - 1))
    take(e_recv, e_ssem, 4 * (sp_n - 1) * seqs)
    take(m_recv, m_ssem, 8 * (sp_n - 1) * seqs)
    pltpu.make_async_copy(view, view, o_ssem).wait()


def unpack(packed, mem_out, norm_out, peak_out, read_out):
    seqs = mem_out.shape[0]
    for s in range(seqs):
        rows = packed[8 * s : 8 * s + 8, :]
        mem_out[s, 0] = rows[:, 0:64].astype(BF16)
        mem_out[s, 1] = rows[:, 64:128].astype(BF16)
        norm = packed[32 + s : 33 + s, :]
        norm_out[s, 0:1, :] = norm[:, 0:4].astype(BF16)
        norm_out[s, 1:2, :] = norm[:, 64:68].astype(BF16)
        peak = packed[36 + s : 37 + s, :]
        peak_out[0:1, s : s + 1] = peak[:, 0:1]
        peak_out[1:2, s : s + 1] = peak[:, 64:65]
    read_out[...] = packed[40:44, 0:32].astype(BF16)


def body(
    prompt, key_weight, value_weight, input_gate_weight, forget_gate_weight, forget_bias,
    key_taps, extra_decay, new_query, new_key, new_value, new_input_gate, new_forget_gate,
    out_weight,
):
    seqs, length, width = prompt.shape
    sp_n = lax.axis_size("sp")
    tp_n = lax.axis_size("tp")
    cols_of = out_weight.shape[2] // sp_n
    any_spec = pl.BlockSpec(memory_space=pl.ANY)
    vmem = pl.BlockSpec(memory_space=pltpu.VMEM)
    dma = pltpu.SemaphoreType.DMA
    packed = pl.pallas_call(
        kernel,
        out_shape=pltpu.VMEM((48, 128), F32),
        in_specs=[any_spec] * 14,
        out_specs=vmem,
        scratch_shapes=[
            pltpu.VMEM((seqs, length, width), BF16),
            pltpu.VMEM((width, 128), BF16),
            pltpu.VMEM((width, 256), BF16),
            pltpu.VMEM((400, width), BF16),
            pltpu.VMEM((64, width), BF16),
            pltpu.VMEM((seqs, 400, length), F32),
            pltpu.VMEM((length, length), BF16),
            pltpu.VMEM((4, 8, 128), F32),
            pltpu.VMEM((seqs * 128, 128), F32),
            pltpu.VMEM((seqs * 4, 128), F32),
            pltpu.VMEM((2, 8, 128), F32),
            pltpu.VMEM((2, 8, 128), F32),
            pltpu.VMEM((seqs * sp_n * 4, 128), F32),
            pltpu.VMEM((seqs * sp_n * 8, 128), F32),
            pltpu.VMEM((2, 2, 8, 8, cols_of), BF16),
            pltpu.VMEM((2, 4, 128), F32),
            pltpu.VMEM((tp_n, 4, 128), F32),
            pltpu.VMEM((8, 128), F32),
            pltpu.VMEM((sp_n * 8, 128), F32),
            pltpu.VMEM((seqs, 272, length), BF16),
            pltpu.VMEM((seqs, 128, length), BF16),
            pltpu.VMEM((seqs, 16, length), BF16),
            pltpu.VMEM((seqs, 4, length), F32),
            pltpu.VMEM((256, cols_of), BF16),
            pltpu.VMEM((128, 128), F32),
            pltpu.VMEM((2, width), BF16),
            pltpu.VMEM((2, width), BF16),
            pltpu.SMEM((2,), F32),
            pltpu.VMEM((3, 128), BF16),
            pltpu.VMEM((seqs, 2, length), F32),
            pltpu.VMEM((seqs, 2, 64), BF16),
            pltpu.VMEM((seqs, 2, 64), BF16),
            pltpu.VMEM((seqs, 2, 8), BF16),
            pltpu.VMEM((2, seqs), F32),
            pltpu.VMEM((2, seqs), F32),
            dma((1 + CHUNKS,)),
            dma((CHUNKS + seqs,)),
            dma,
            dma((10,)),
            dma,
            dma,
            dma,
            dma,
            dma((2,)),
            dma,
            dma,
            dma,
            dma,
            dma,
            dma,
            dma,
            dma,
        ],
        compiler_params=pltpu.CompilerParams(
            collective_id=0, has_side_effects=True, vmem_limit_bytes=60 * 1024 * 1024
        ),
        name="prompt_state",
    )(
        prompt,
        key_weight,
        value_weight,
        input_gate_weight.T,
        forget_gate_weight.T,
        forget_bias,
        key_taps,
        jnp.transpose(extra_decay, (0, 2, 1)),
        new_query,
        new_key,
        new_value,
        new_input_gate.T,
        new_forget_gate.T,
        out_weight,
    )
    memory, norm, peak, read = pl.pallas_call(
        unpack,
        out_shape=(
            jax.ShapeDtypeStruct((seqs, 2, 8, 64), BF16),
            jax.ShapeDtypeStruct((seqs, 2, 4), BF16),
            jax.ShapeDtypeStruct((2, seqs), F32),
            jax.ShapeDtypeStruct((seqs, 32), BF16),
        ),
        in_specs=[vmem],
        out_specs=(vmem,) * 4,
        compiler_params=pltpu.CompilerParams(vmem_limit_bytes=1024 * 1024),
        name="unpack",
    )(packed)
    return jnp.transpose(memory, (0, 1, 3, 2)), norm, peak.T, read


def solution(mesh):
    in_specs = (
        P(None, "sp", None),
        P(None, "tp"),
        P(None, "tp"),
        P(None, "tp"),
        P(None, "tp"),
        P("tp"),
        P(None, "tp"),
        P(None, "sp", "tp"),
        P(None, "tp", None),
        P(None, "tp", None),
        P(None, "tp", "sp"),
        P(None, "tp"),
        P(None, "tp"),
        P("tp", "sp", None),
    )
    out_specs = (
        P(None, "tp", None, "sp"),
        P(None, "tp", "sp"),
        P(None, "tp"),
        P(None, ("sp", "tp")),
    )
    return jax.shard_map(body, mesh=mesh, in_specs=in_specs, out_specs=out_specs, check_vma=False)
```

```python
import jax
import jax.numpy as jnp
from jax import lax
from jax.experimental import pallas as pl
from jax.experimental.pallas import tpu as pltpu
from jax.sharding import PartitionSpec as P

MESH_ID = pl.DeviceIdType.MESH
F32 = jnp.float32
BF16 = jnp.bfloat16
NT = (((1,), (1,)), ((), ()))
KEY0 = 16
VAL0 = 144
CHUNKS = 4


def log_sigmoid(x):
    return jnp.minimum(x, 0.0) - jnp.log1p(jnp.exp(-jnp.abs(x)))


def three_parts(x):
    high = x.astype(BF16)
    rest = x - high.astype(F32)
    middle = rest.astype(BF16)
    low = (rest - middle.astype(F32)).astype(BF16)
    return high, middle, low


def kernel(
    prompt, key_w, value_w, in_w, fg_w, fg_bias, taps, extra, query, new_key, new_value,
    new_in, new_fg, out_w,
    packed,
    p_buf, wk_buf, wv_buf, wt_buf, hp_buf, r_buf, tri_buf, par_buf, mem_buf, e_buf,
    h_send, h_recv, e_recv, m_recv, ow_recv, part_buf, part_recv, f_buf, f_recv, lhs_buf, key_buf,
    along_buf, suf_buf, ow_buf, col_buf,
    in_v, fg_v, bias_v, taps_v, extra_v, query_v, key_v, value_v, nin_v, nfg_v,
    w_sem, p_sem, hp_sem, small_sem, ow_local, h_ssem, h_rsem, e_ssem, e_rsem, m_ssem, m_rsem,
    ow_ssem, ow_rsem, o_ssem, o_rsem, f_ssem, f_rsem,
):
    seqs, length, width = p_buf.shape
    sp_n, tp_n = lax.axis_size("sp"), lax.axis_size("tp")
    sp, tp = lax.axis_index("sp"), lax.axis_index("tp")
    step = width // CHUNKS

    barrier = pltpu.get_barrier_semaphore()

    def sp_peer(d):
        return lax.rem(sp + d, sp_n)

    def tp_peer(d):
        return lax.rem(tp + d, tp_n)

    small_pairs = (
        (in_w, in_v), (fg_w, fg_v), (fg_bias, bias_v), (taps, taps_v), (extra, extra_v),
        (query, query_v), (new_key, key_v), (new_value, value_v), (new_in, nin_v),
        (new_fg, nfg_v),
    )
    small_copies = [
        pltpu.make_async_copy(src, dst, small_sem.at[i])
        for i, (src, dst) in enumerate(small_pairs)
    ]
    hp_copies = []
    for s in range(seqs):
        for side, row in ((0, 0), (1, length - 8)):
            g = 2 * s + side
            hp_copies.append(
                pltpu.make_async_copy(
                    prompt.at[s, pl.ds(row, 8), :], hp_buf.at[pl.ds(8 * g, 8), :], hp_sem
                )
            )
    wk_copies = [
        pltpu.make_async_copy(key_w.at[rows, :], wk_buf.at[rows, :], w_sem.at[0])
        for rows in (pl.ds(0, width // 2), pl.ds(width // 2, width // 2))
    ]
    w_copies, p_copies = [], []
    for c in range(CHUNKS):
        rows = pl.ds(c * step, step)
        w_copies.append(
            pltpu.make_async_copy(value_w.at[rows, :], wv_buf.at[rows, :], w_sem.at[1 + c])
        )
        p_copies.append(
            pltpu.make_async_copy(prompt.at[0, :, rows], p_buf.at[0, :, rows], p_sem.at[c])
        )
    s_copies = [p_copies]
    for s in range(1, seqs):
        group = []
        for c in range(CHUNKS):
            cols = pl.ds(c * step, step)
            s_sem = p_sem.at[CHUNKS + c // 2 if s == 1 else CHUNKS + s]
            group.append(
                pltpu.make_async_copy(prompt.at[s, :, cols], p_buf.at[s, :, cols], s_sem)
            )
        s_copies.append(group)

    def start(copies, priority=0):
        for copy in copies:
            copy.start(priority=priority)

    def finished(copies):
        for copy in copies:
            copy.wait()

    def landed(view, sem):
        pltpu.make_async_copy(view, view, sem).wait()

    start(wk_copies)
    start(hp_copies)
    start(w_copies[:1])
    start(p_copies[:1])
    start(small_copies)
    start(w_copies[1:2], 1)
    start(p_copies[1:2], 1)
    start(w_copies[2:3], 1)
    start(p_copies[2:3], 1)

    @pl.loop(1, sp_n)
    def _(d):
        pl.semaphore_signal(barrier, inc=1, device_id=(sp_peer(d), tp), device_id_type=MESH_ID)

    @pl.loop(1, tp_n)
    def _(d):
        pl.semaphore_signal(barrier, inc=1, device_id=(sp, tp_peer(d)), device_id_type=MESH_ID)

    tri_buf[...] = (
        lax.broadcasted_iota(jnp.int32, (length, length), 0)
        > lax.broadcasted_iota(jnp.int32, (length, length), 1)
    ).astype(F32).astype(BF16)

    lane = lax.broadcasted_iota(jnp.int32, (1, 128), 1)
    first_head = lane < 64

    def halves(left, right):
        return jnp.where(first_head, left, right)

    def chunk_of(c):
        return pl.ds(c * step, step)

    def turn(c):
        cols = chunk_of(c)
        wt_buf[KEY0:VAL0, cols] = jnp.transpose(wk_buf[cols, :])
        wt_buf[VAL0:, cols] = jnp.transpose(wv_buf[cols, :])

    def chunk_dot(s, c):
        cols = chunk_of(c)
        part = lax.dot_general(
            wt_buf[:, cols], p_buf[s, :, cols], NT, preferred_element_type=F32
        )
        if c == 0:
            r_buf[s] = part
        else:
            r_buf[s] = r_buf[s] + part

    landed(wk_buf, w_sem.at[0])
    landed(hp_buf, hp_sem)
    finished(small_copies)
    finished(w_copies[:1])
    start(w_copies[3:], 1)
    start(p_copies[3:], 1)
    start(s_copies[1][:2], 1)
    edge = jnp.dot(hp_buf[...], wk_buf[...], preferred_element_type=F32).astype(BF16).astype(F32)
    zero4 = jnp.zeros((4, 128), F32)
    h_send[0] = jnp.concatenate(
        [edge[16 * s + 15 : 16 * s + 16] for s in range(seqs)] + [zero4], axis=0
    )
    h_send[1] = jnp.concatenate(
        [edge[16 * s : 16 * s + 1] for s in range(seqs)] + [zero4], axis=0
    )

    gate_rows = jnp.concatenate(
        [
            in_v[...].astype(F32), jnp.zeros((6, width), F32),
            fg_v[...].astype(F32), jnp.zeros((6, width), F32),
        ],
        axis=0,
    )
    wt_buf[0:KEY0, :] = gate_rows.astype(BF16)
    turn(0)

    finished(p_copies[:1])
    finished(w_copies[1:2])
    start(s_copies[1][2:], 1)
    chunk_dot(0, 0)
    turn(1)
    pl.semaphore_wait(barrier, sp_n - 1 + tp_n - 1)
    for side, d in ((0, 1), (1, sp_n - 1)):
        copy = pltpu.make_async_remote_copy(
            src_ref=h_send.at[side],
            dst_ref=h_recv.at[side],
            send_sem=h_ssem,
            recv_sem=h_rsem,
            device_id=(sp_peer(d), tp),
            device_id_type=MESH_ID,
        )
        copy.start()

    finished(p_copies[1:2])
    finished(w_copies[2:3])
    chunk_dot(0, 1)
    turn(2)
    finished(p_copies[2:3])
    finished(w_copies[3:])
    start(s_copies[2], 1)
    chunk_dot(0, 2)
    turn(3)

    for s in range(seqs):
        rows = pl.ds(s, 1)
        par_buf[0, rows, :] = jnp.concatenate(
            [query_v[s, 0:1, :].astype(F32), query_v[s, 1:2, :].astype(F32)], axis=1
        )
        par_buf[1, rows, :] = jnp.concatenate(
            [key_v[s, 0:1, :].astype(F32), key_v[s, 1:2, :].astype(F32)], axis=1
        )
        par_buf[2, rows, :] = halves(nin_v[0:1, s : s + 1], nin_v[1:2, s : s + 1])
        par_buf[3, rows, :] = halves(nfg_v[0:1, s : s + 1], nfg_v[1:2, s : s + 1])
        fresh = value_v[s].astype(F32)
        spread = jnp.concatenate([fresh, jnp.zeros((2, 120), F32)], axis=1)
        left = pltpu.roll(spread, 8 * lax.rem(sp, 8), 1)
        fresh_row = halves(left[0:1], pltpu.roll(left[1:2], 64, 1))
        f_buf[s : s + 1, :] = jnp.where(sp < 8, fresh_row, 0.0)
        f_buf[4 + s : 5 + s, :] = jnp.where(sp < 8, 0.0, fresh_row)
    col_buf[:, 0:8] = jnp.transpose(
        jnp.concatenate(
            [taps_v[...].astype(F32), jnp.zeros((1, 128), F32), par_buf[0, 0:4, :]], axis=0
        )
    )

    bias_col = jnp.where(
        lax.broadcasted_iota(jnp.int32, (2, 1), 0) == 0, bias_v[0], bias_v[1]
    )

    cols_of = out_w.shape[2] // sp_n

    def ow_slot(ref):
        return ref.at[sp // 8, :, lax.rem(sp, 8)]

    def ow_cols(j):
        return out_w.at[:, :, pl.ds(pl.multiple_of(j * cols_of, cols_of), cols_of)]

    pos = lax.broadcasted_iota(jnp.int32, (1, length), 1)
    my_rows = pl.multiple_of(8 * sp, 8)
    my_tile = pl.multiple_of(8 * sp, 8)

    def slot_rows(s, size):
        return pl.ds(pl.multiple_of((s * sp_n + sp) * size, size), size)

    def rows_of(x):
        parts = [part.astype(F32) for part in three_parts(x)]
        return jnp.concatenate(parts + [jnp.zeros((10, length), F32)], axis=0).astype(BF16)

    def joined(x, h):
        return x[h : h + 1] + x[2 + h : 3 + h] + x[4 + h : 5 + h]

    def suffix(s):
        fg_pre = r_buf[s, 8:10, :].astype(BF16).astype(F32)
        log_f = log_sigmoid(fg_pre + bias_col) + extra_v[s]
        if s == seqs - 1:
            sums = jnp.dot(rows_of(log_f), tri_buf[...], preferred_element_type=F32)
            later = sums[0:2] + sums[2:4] + sums[4:6]
        else:
            later = jnp.where(pos < length - 1, pltpu.roll(log_f, length - 1, 1), 0.0)
            shift = 1
            while shift < length:
                later = later + jnp.where(
                    pos < length - shift, pltpu.roll(later, length - shift, 1), 0.0
                )
                shift *= 2
        suf_buf[s, 0:2, :] = later
        suf_buf[s, 2:4, :] = jnp.broadcast_to(later[:, 0:1] + log_f[:, 0:1], (2, length))

    def keys(s):
        key = r_buf[s, KEY0:VAL0, :].astype(BF16).astype(F32)
        edge = length - 128
        earlier = pltpu.roll(key, 1, 1)
        earlier = jnp.concatenate(
            [jnp.where(lane == 0, col_buf[:, 8 + s : 9 + s], earlier[:, :128]), earlier[:, 128:]],
            axis=1,
        )
        coming = pltpu.roll(key, length - 1, 1)
        coming = jnp.concatenate(
            [
                coming[:, :edge],
                jnp.where(lane == 127, col_buf[:, 16 + s : 17 + s], coming[:, edge:]),
            ],
            axis=1,
        )
        mixed = col_buf[:, 0:1] * earlier + col_buf[:, 1:2] * key + col_buf[:, 2:3] * coming
        key_rows = (mixed * jax.nn.sigmoid(mixed) * 0.125).astype(BF16)
        key_buf[s] = key_rows
        prod = key_rows.astype(F32) * col_buf[:, 4 + s : 5 + s]
        along = jnp.concatenate(
            [
                jnp.sum(prod[0:64], axis=0, keepdims=True),
                jnp.sum(prod[64:128], axis=0, keepdims=True),
            ],
            axis=0,
        )
        along_buf[s] = rows_of(along)

    def weigh(s):
        in_pre = r_buf[s, 0:2, :].astype(BF16).astype(F32)
        gate = in_pre + suf_buf[s, 0:2, :]
        top = jnp.max(gate, axis=1, keepdims=True)
        scale = jnp.exp(gate - top)
        lhs_buf[s, 0:16, :] = rows_of(scale)
        for h in range(2):
            value = r_buf[s, VAL0 + 128 * h : VAL0 + 128 * (h + 1), :].astype(BF16).astype(F32)
            lhs_buf[s, 16 + 128 * h : 144 + 128 * h, :] = (value * scale[h : h + 1]).astype(BF16)
        total = suf_buf[s, 2:4, 0:1]
        row = jnp.where(
            lax.rem(lane, 64) < 32,
            halves(total[0:1], total[1:2]),
            halves(top[0:1], top[1:2]),
        )
        e_buf[4 * s + 3 : 4 * s + 4, :] = row

    def outer(s):
        num_parts = lax.dot_general(
            along_buf[s], lhs_buf[s, 16:, :], NT, preferred_element_type=F32
        )
        both = lax.dot_general(lhs_buf[s], key_buf[s], NT, preferred_element_type=F32)
        num0 = joined(num_parts, 0)[:, 0:128]
        num1 = joined(num_parts, 1)[:, 128:256]
        e_buf[4 * s : 4 * s + 1, :] = halves(joined(both, 0), joined(both, 1))
        e_buf[4 * s + 1 : 4 * s + 2, :] = halves(num0, pltpu.roll(num1, 64, 1))
        e_buf[4 * s + 2 : 4 * s + 3, :] = halves(pltpu.roll(num0, 64, 1), num1)
        mem_buf[pl.ds(128 * s, 128), :] = halves(both[16:144], both[144:272])

    z, x = sp // 4, lax.rem(sp, 4)
    offsets = sorted(
        ((dz, dx) for dz in range(4) for dx in range(4) if dz or dx),
        key=lambda o: -(min(o[0], 4 - o[0]) + min(o[1], 4 - o[1])),
    )
    peers = [lax.rem(z + dz, 4) * 4 + lax.rem(x + dx, 4) for dz, dx in offsets]

    def send_sums(s):
        e_recv[slot_rows(s, 4), :] = e_buf[4 * s : 4 * s + 4, :]
        for j in peers:
            pltpu.make_async_remote_copy(
                src_ref=e_buf.at[pl.ds(4 * s, 4), :],
                dst_ref=e_recv.at[slot_rows(s, 4), :],
                send_sem=e_ssem,
                recv_sem=e_rsem.at[s // (seqs - 1)],
                device_id=(j, tp),
                device_id_type=MESH_ID,
            ).start()

    def send_memory(s):
        m_recv[slot_rows(s, 8), :] = mem_buf[pl.ds(128 * s + my_rows, 8), :]
        for j in peers:
            pltpu.make_async_remote_copy(
                src_ref=mem_buf.at[pl.ds(pl.multiple_of(128 * s + 8 * j, 8), 8), :],
                dst_ref=m_recv.at[slot_rows(s, 8), :],
                send_sem=m_ssem,
                recv_sem=m_rsem,
                device_id=(j, tp),
                device_id_type=MESH_ID,
            ).start()

    finished(p_copies[3:])
    landed(p_buf.at[1, :, pl.ds(0, width // 2)], p_sem.at[CHUNKS])
    start(s_copies[3], 1)
    chunk_dot(0, 3)
    chunk_dot(1, 0)
    chunk_dot(1, 1)
    suffix(0)
    landed(p_buf.at[1, :, pl.ds(width // 2, width // 2)], p_sem.at[CHUNKS + 1])
    chunk_dot(1, 2)
    chunk_dot(1, 3)

    landed(h_recv, h_rsem)
    landed(p_buf.at[2], p_sem.at[CHUNKS + 2])
    col_buf[:, 8:16] = jnp.where(sp == 0, 0.0, jnp.transpose(h_recv[0]))
    col_buf[:, 16:24] = jnp.where(sp == sp_n - 1, 0.0, jnp.transpose(h_recv[1]))
    chunk_dot(2, 0)
    own_ow = pltpu.make_async_copy(ow_cols(sp), ow_slot(ow_recv), ow_local)
    own_ow.start()
    f_recv[pl.ds(my_tile, 8), :] = f_buf[...]
    for j in peers:
        pltpu.make_async_remote_copy(
            src_ref=f_buf,
            dst_ref=f_recv.at[pl.ds(my_tile, 8), :],
            send_sem=f_ssem,
            recv_sem=f_rsem,
            device_id=(j, tp),
            device_id_type=MESH_ID,
        ).start()
        pltpu.make_async_remote_copy(
            src_ref=ow_cols(j),
            dst_ref=ow_slot(ow_recv),
            send_sem=ow_ssem,
            recv_sem=ow_rsem,
            device_id=(j, tp),
            device_id_type=MESH_ID,
        ).start()

    chunk_dot(2, 1)
    keys(0)
    weigh(0)
    chunk_dot(2, 2)
    suffix(1)
    chunk_dot(2, 3)

    landed(p_buf.at[3], p_sem.at[CHUNKS + 3])
    outer(0)
    chunk_dot(3, 0)
    keys(1)
    weigh(1)
    send_sums(0)
    send_memory(0)
    chunk_dot(3, 1)
    suffix(2)
    outer(1)
    chunk_dot(3, 2)
    keys(2)
    weigh(2)
    send_sums(1)
    chunk_dot(3, 3)
    outer(2)
    suffix(3)
    send_sums(2)
    keys(3)
    weigh(3)
    outer(3)
    send_sums(3)
    send_memory(1)
    send_memory(2)
    send_memory(3)

    def take(ref, sem, count):
        view = ref.at[pl.ds(0, count), :]
        pltpu.make_async_copy(view, view, sem).wait()

    own_ow.wait()
    ow_bytes = out_w.at[:, :, pl.ds(0, cols_of * (sp_n - 1))]
    pltpu.make_async_copy(ow_bytes, ow_bytes, ow_rsem).wait()
    ow_buf[...] = ow_recv[...].reshape(256, cols_of)
    take(f_recv, f_rsem, 8 * (sp_n - 1))
    fresh_sum = f_recv[0:8, :]
    for i in range(1, sp_n):
        fresh_sum = fresh_sum + f_recv[8 * i : 8 * i + 8, :]

    row16 = lax.broadcasted_iota(jnp.int32, (sp_n, 128), 0)
    low_lanes = lax.rem(lax.broadcasted_iota(jnp.int32, (sp_n, 128), 1), 64) < 32

    def by_head(x):
        left = jnp.sum(jnp.where(first_head, x, 0.0), axis=1, keepdims=True)
        right = jnp.sum(jnp.where(first_head, 0.0, x), axis=1, keepdims=True)
        return halves(left, right)

    def combine(s):
        def rows_at(k):
            return e_recv[pl.ds(s * sp_n * 4 + k, sp_n, stride=4), :]

        stats = rows_at(3)
        totals = jnp.where(low_lanes, stats, pltpu.roll(stats, 32, 1))
        tops = jnp.where(low_lanes, pltpu.roll(stats, 96, 1), stats)
        later = jnp.where(row16 < sp_n - 1, pltpu.roll(totals, sp_n - 1, 0), 0.0)
        shift = 1
        while shift < sp_n:
            later = later + jnp.where(
                row16 < sp_n - shift, pltpu.roll(later, sp_n - shift, 0), 0.0
            )
            shift *= 2
        gate = tops + later
        peak = jnp.max(gate, axis=0, keepdims=True)
        factor = jnp.exp(gate - peak)

        def summed(k):
            return jnp.sum(factor * rows_at(k), axis=0, keepdims=True)

        norm, num_a, num_b = summed(0), summed(1), summed(2)
        q, k = par_buf[0, s : s + 1, :], par_buf[1, s : s + 1, :]
        gate_in, gate_fg = par_buf[2, s : s + 1, :], par_buf[3, s : s + 1, :]
        kept = log_sigmoid(gate_fg) + peak
        new_peak = jnp.maximum(kept, gate_in)
        old_scale = jnp.exp(kept - new_peak)
        new_scale = jnp.exp(gate_in - new_peak)
        denom = jnp.maximum(jnp.abs(by_head(q * (old_scale * norm + new_scale * k))), 1.0)
        fresh_scale = new_scale * by_head(q * k)
        read_a = (old_scale * num_a + fresh_scale * fresh_sum[s : s + 1]) / denom
        read_b = (old_scale * num_b + fresh_scale * fresh_sum[4 + s : 5 + s]) / denom
        packed[32 + s : 33 + s, :] = pltpu.roll(norm, lax.rem(128 - 4 * sp, 128), 1)
        packed[36 + s : 37 + s, :] = peak
        return jnp.concatenate([read_a, read_b], axis=1), factor

    reads, factors = [], []
    take(e_recv, e_rsem.at[0], 4 * (sp_n - 1) * (seqs - 1))
    for s in range(seqs - 1):
        row, factor = combine(s)
        reads.append(row)
        factors.append(factor)
    take(e_recv, e_rsem.at[1], 4 * (sp_n - 1))
    row, factor = combine(seqs - 1)
    reads.append(row)
    factors.append(factor)

    read = jnp.concatenate(reads + [jnp.zeros((12, 256), F32)], axis=0).astype(BF16)
    part = jnp.dot(read, ow_buf[...], preferred_element_type=F32)[0:4]
    part_buf[0] = part[:, 0:128]
    part_buf[1] = part[:, 128:256]
    part_recv[tp] = part_buf[tp // 4]
    y, core = tp // 2, lax.rem(tp, 2)
    for dy, dc in ((2, 1), (2, 0), (1, 1), (3, 1), (1, 0), (3, 0), (0, 1)):
        j = lax.rem(y + dy, 4) * 2 + lax.rem(core + dc, 2)
        pltpu.make_async_remote_copy(
            src_ref=part_buf.at[j // 4],
            dst_ref=part_recv.at[tp],
            send_sem=o_ssem,
            recv_sem=o_rsem,
            device_id=(sp, j),
            device_id_type=MESH_ID,
        ).start()

    take(m_recv, m_rsem, 8 * (sp_n - 1) * seqs)
    for s in range(seqs):
        memory = jnp.zeros((8, 128), F32)
        for i in range(sp_n):
            base = (s * sp_n + i) * 8
            memory = memory + factors[s][i : i + 1] * m_recv[base : base + 8, :]
        packed[8 * s : 8 * s + 8, :] = memory

    view = part_recv.at[pl.ds(0, tp_n - 1)]
    pltpu.make_async_copy(view, view, o_rsem).wait()
    whole = part_recv[0]
    for i in range(1, tp_n):
        whole = whole + part_recv[i]
    packed[40:44, :] = pltpu.roll(whole, lax.rem(128 - 32 * lax.rem(tp, 4), 128), 1)

    landed(h_recv, h_ssem)
    pltpu.make_async_copy(ow_bytes, ow_bytes, ow_ssem).wait()
    take(f_recv, f_ssem, 8 * (sp_n - 1))
    take(e_recv, e_ssem, 4 * (sp_n - 1) * seqs)
    take(m_recv, m_ssem, 8 * (sp_n - 1) * seqs)
    pltpu.make_async_copy(view, view, o_ssem).wait()


def unpack(packed, mem_out, norm_out, peak_out, read_out):
    seqs = mem_out.shape[0]
    for s in range(seqs):
        rows = packed[8 * s : 8 * s + 8, :]
        mem_out[s, 0] = rows[:, 0:64].astype(BF16)
        mem_out[s, 1] = rows[:, 64:128].astype(BF16)
        norm = packed[32 + s : 33 + s, :]
        norm_out[s, 0:1, :] = norm[:, 0:4].astype(BF16)
        norm_out[s, 1:2, :] = norm[:, 64:68].astype(BF16)
        peak = packed[36 + s : 37 + s, :]
        peak_out[0:1, s : s + 1] = peak[:, 0:1]
        peak_out[1:2, s : s + 1] = peak[:, 64:65]
    read_out[...] = packed[40:44, 0:32].astype(BF16)


def body(
    prompt, key_weight, value_weight, input_gate_weight, forget_gate_weight, forget_bias,
    key_taps, extra_decay, new_query, new_key, new_value, new_input_gate, new_forget_gate,
    out_weight,
):
    seqs, length, width = prompt.shape
    sp_n = lax.axis_size("sp")
    tp_n = lax.axis_size("tp")
    cols_of = out_weight.shape[2] // sp_n
    any_spec = pl.BlockSpec(memory_space=pl.ANY)
    vmem = pl.BlockSpec(memory_space=pltpu.VMEM)
    dma = pltpu.SemaphoreType.DMA
    packed = pl.pallas_call(
        kernel,
        out_shape=pltpu.VMEM((48, 128), F32),
        in_specs=[any_spec] * 14,
        out_specs=vmem,
        scratch_shapes=[
            pltpu.VMEM((seqs, length, width), BF16),
            pltpu.VMEM((width, 128), BF16),
            pltpu.VMEM((width, 256), BF16),
            pltpu.VMEM((400, width), BF16),
            pltpu.VMEM((64, width), BF16),
            pltpu.VMEM((seqs, 400, length), F32),
            pltpu.VMEM((length, length), BF16),
            pltpu.VMEM((4, 8, 128), F32),
            pltpu.VMEM((seqs * 128, 128), F32),
            pltpu.VMEM((seqs * 4, 128), F32),
            pltpu.VMEM((2, 8, 128), F32),
            pltpu.VMEM((2, 8, 128), F32),
            pltpu.VMEM((seqs * sp_n * 4, 128), F32),
            pltpu.VMEM((seqs * sp_n * 8, 128), F32),
            pltpu.VMEM((2, 2, 8, 8, cols_of), BF16),
            pltpu.VMEM((2, 4, 128), F32),
            pltpu.VMEM((tp_n, 4, 128), F32),
            pltpu.VMEM((8, 128), F32),
            pltpu.VMEM((sp_n * 8, 128), F32),
            pltpu.VMEM((seqs, 272, length), BF16),
            pltpu.VMEM((seqs, 128, length), BF16),
            pltpu.VMEM((seqs, 16, length), BF16),
            pltpu.VMEM((seqs, 4, length), F32),
            pltpu.VMEM((256, cols_of), BF16),
            pltpu.VMEM((128, 128), F32),
            pltpu.VMEM((2, width), BF16),
            pltpu.VMEM((2, width), BF16),
            pltpu.SMEM((2,), F32),
            pltpu.VMEM((3, 128), BF16),
            pltpu.VMEM((seqs, 2, length), F32),
            pltpu.VMEM((seqs, 2, 64), BF16),
            pltpu.VMEM((seqs, 2, 64), BF16),
            pltpu.VMEM((seqs, 2, 8), BF16),
            pltpu.VMEM((2, seqs), F32),
            pltpu.VMEM((2, seqs), F32),
            dma((1 + CHUNKS,)),
            dma((CHUNKS + seqs,)),
            dma,
            dma((10,)),
            dma,
            dma,
            dma,
            dma,
            dma((2,)),
            dma,
            dma,
            dma,
            dma,
            dma,
            dma,
            dma,
            dma,
        ],
        compiler_params=pltpu.CompilerParams(
            collective_id=0, has_side_effects=True, vmem_limit_bytes=60 * 1024 * 1024
        ),
        name="prompt_state",
    )(
        prompt,
        key_weight,
        value_weight,
        input_gate_weight.T,
        forget_gate_weight.T,
        forget_bias,
        key_taps,
        jnp.transpose(extra_decay, (0, 2, 1)),
        new_query,
        new_key,
        new_value,
        new_input_gate.T,
        new_forget_gate.T,
        out_weight,
    )
    memory, norm, peak, read = pl.pallas_call(
        unpack,
        out_shape=(
            jax.ShapeDtypeStruct((seqs, 2, 8, 64), BF16),
            jax.ShapeDtypeStruct((seqs, 2, 4), BF16),
            jax.ShapeDtypeStruct((2, seqs), F32),
            jax.ShapeDtypeStruct((seqs, 32), BF16),
        ),
        in_specs=[vmem],
        out_specs=(vmem,) * 4,
        compiler_params=pltpu.CompilerParams(vmem_limit_bytes=1024 * 1024),
        name="unpack",
    )(packed)
    return jnp.transpose(memory, (0, 1, 3, 2)), norm, peak.T, read


def solution(mesh):
    in_specs = (
        P(None, "sp", None),
        P(None, "tp"),
        P(None, "tp"),
        P(None, "tp"),
        P(None, "tp"),
        P("tp"),
        P(None, "tp"),
        P(None, "sp", "tp"),
        P(None, "tp", None),
        P(None, "tp", None),
        P(None, "tp", "sp"),
        P(None, "tp"),
        P(None, "tp"),
        P("tp", "sp", None),
    )
    out_specs = (
        P(None, "tp", None, "sp"),
        P(None, "tp", "sp"),
        P(None, "tp"),
        P(None, ("sp", "tp")),
    )
    return jax.shard_map(body, mesh=mesh, in_specs=in_specs, out_specs=out_specs, check_vma=False)
```

```python
import jax
import jax.numpy as jnp
from jax import lax
from jax.experimental import pallas as pl
from jax.experimental.pallas import tpu as pltpu
from jax.sharding import PartitionSpec as P

MESH_ID = pl.DeviceIdType.MESH
F32 = jnp.float32
BF16 = jnp.bfloat16
NT = (((1,), (1,)), ((), ()))
KEY0 = 16
VAL0 = 144
CHUNKS = 4


def log_sigmoid(x):
    return jnp.minimum(x, 0.0) - jnp.log1p(jnp.exp(-jnp.abs(x)))


def three_parts(x):
    high = x.astype(BF16)
    rest = x - high.astype(F32)
    middle = rest.astype(BF16)
    low = (rest - middle.astype(F32)).astype(BF16)
    return high, middle, low


def kernel(
    prompt, key_w, value_w, in_w, fg_w, fg_bias, taps, extra, query, new_key, new_value,
    new_in, new_fg, out_w,
    packed,
    p_buf, wk_buf, wv_buf, wt_buf, hp_buf, r_buf, tri_buf, par_buf, mem_buf, e_buf,
    h_send, h_recv, e_recv, m_recv, ow_recv, part_buf, part_recv, f_buf, f_recv, lhs_buf, key_buf,
    along_buf, suf_buf, ow_buf, col_buf,
    in_v, fg_v, bias_v, taps_v, extra_v, query_v, key_v, value_v, nin_v, nfg_v,
    w_sem, p_sem, hp_sem, small_sem, ow_local, h_ssem, h_rsem, e_ssem, e_rsem, m_ssem, m_rsem,
    ow_ssem, ow_rsem, o_ssem, o_rsem, f_ssem, f_rsem,
):
    seqs, length, width = p_buf.shape
    sp_n, tp_n = lax.axis_size("sp"), lax.axis_size("tp")
    sp, tp = lax.axis_index("sp"), lax.axis_index("tp")
    step = width // CHUNKS

    barrier = pltpu.get_barrier_semaphore()

    def sp_peer(d):
        return lax.rem(sp + d, sp_n)

    def tp_peer(d):
        return lax.rem(tp + d, tp_n)

    small_pairs = (
        (in_w, in_v), (fg_w, fg_v), (fg_bias, bias_v), (taps, taps_v), (extra, extra_v),
        (query, query_v), (new_key, key_v), (new_value, value_v), (new_in, nin_v),
        (new_fg, nfg_v),
    )
    small_copies = [
        pltpu.make_async_copy(src, dst, small_sem.at[i])
        for i, (src, dst) in enumerate(small_pairs)
    ]
    hp_copies = []
    for s in range(seqs):
        for side, row in ((0, 0), (1, length - 8)):
            g = 2 * s + side
            hp_copies.append(
                pltpu.make_async_copy(
                    prompt.at[s, pl.ds(row, 8), :], hp_buf.at[pl.ds(8 * g, 8), :], hp_sem
                )
            )
    wk_copies = [
        pltpu.make_async_copy(key_w.at[rows, :], wk_buf.at[rows, :], w_sem.at[0])
        for rows in (pl.ds(0, width // 2), pl.ds(width // 2, width // 2))
    ]
    w_copies, p_copies = [], []
    for c in range(CHUNKS):
        rows = pl.ds(c * step, step)
        w_copies.append(
            pltpu.make_async_copy(value_w.at[rows, :], wv_buf.at[rows, :], w_sem.at[1 + c])
        )
        p_copies.append(
            pltpu.make_async_copy(prompt.at[0, :, rows], p_buf.at[0, :, rows], p_sem.at[c])
        )
    s_copies = [p_copies]
    for s in range(1, seqs):
        group = []
        for c in range(CHUNKS):
            cols = pl.ds(c * step, step)
            s_sem = p_sem.at[CHUNKS + c // 2 if s == 1 else CHUNKS + s]
            group.append(
                pltpu.make_async_copy(prompt.at[s, :, cols], p_buf.at[s, :, cols], s_sem)
            )
        s_copies.append(group)

    def start(copies, priority=0):
        for copy in copies:
            copy.start(priority=priority)

    def finished(copies):
        for copy in copies:
            copy.wait()

    def landed(view, sem):
        pltpu.make_async_copy(view, view, sem).wait()

    start(wk_copies)
    start(hp_copies)
    start(w_copies[:1])
    start(p_copies[:1])
    start(small_copies)
    start(w_copies[1:2], 1)
    start(p_copies[1:2], 1)
    start(w_copies[2:3], 1)
    start(p_copies[2:3], 1)

    @pl.loop(1, sp_n)
    def _(d):
        pl.semaphore_signal(barrier, inc=1, device_id=(sp_peer(d), tp), device_id_type=MESH_ID)

    @pl.loop(1, tp_n)
    def _(d):
        pl.semaphore_signal(barrier, inc=1, device_id=(sp, tp_peer(d)), device_id_type=MESH_ID)

    tri_buf[...] = (
        lax.broadcasted_iota(jnp.int32, (length, length), 0)
        > lax.broadcasted_iota(jnp.int32, (length, length), 1)
    ).astype(F32).astype(BF16)

    lane = lax.broadcasted_iota(jnp.int32, (1, 128), 1)
    first_head = lane < 64

    def halves(left, right):
        return jnp.where(first_head, left, right)

    def chunk_of(c):
        return pl.ds(c * step, step)

    def turn(c):
        cols = chunk_of(c)
        wt_buf[KEY0:VAL0, cols] = jnp.transpose(wk_buf[cols, :])
        wt_buf[VAL0:, cols] = jnp.transpose(wv_buf[cols, :])

    def chunk_dot(s, c):
        cols = chunk_of(c)
        part = lax.dot_general(
            wt_buf[:, cols], p_buf[s, :, cols], NT, preferred_element_type=F32
        )
        if c == 0:
            r_buf[s] = part
        else:
            r_buf[s] = r_buf[s] + part

    landed(wk_buf, w_sem.at[0])
    landed(hp_buf, hp_sem)
    finished(small_copies)
    finished(w_copies[:1])
    start(w_copies[3:], 1)
    start(p_copies[3:], 1)
    start(s_copies[1][:2], 1)
    edge = jnp.dot(hp_buf[...], wk_buf[...], preferred_element_type=F32).astype(BF16).astype(F32)
    zero4 = jnp.zeros((4, 128), F32)
    h_send[0] = jnp.concatenate(
        [edge[16 * s + 15 : 16 * s + 16] for s in range(seqs)] + [zero4], axis=0
    )
    h_send[1] = jnp.concatenate(
        [edge[16 * s : 16 * s + 1] for s in range(seqs)] + [zero4], axis=0
    )

    gate_rows = jnp.concatenate(
        [
            in_v[...].astype(F32), jnp.zeros((6, width), F32),
            fg_v[...].astype(F32), jnp.zeros((6, width), F32),
        ],
        axis=0,
    )
    wt_buf[0:KEY0, :] = gate_rows.astype(BF16)
    turn(0)

    finished(p_copies[:1])
    finished(w_copies[1:2])
    start(s_copies[1][2:], 1)
    chunk_dot(0, 0)
    turn(1)
    pl.semaphore_wait(barrier, sp_n - 1 + tp_n - 1)
    for side, d in ((0, 1), (1, sp_n - 1)):
        copy = pltpu.make_async_remote_copy(
            src_ref=h_send.at[side],
            dst_ref=h_recv.at[side],
            send_sem=h_ssem,
            recv_sem=h_rsem,
            device_id=(sp_peer(d), tp),
            device_id_type=MESH_ID,
        )
        copy.start()

    finished(p_copies[1:2])
    finished(w_copies[2:3])
    chunk_dot(0, 1)
    turn(2)
    finished(p_copies[2:3])
    finished(w_copies[3:])
    start(s_copies[2], 1)
    chunk_dot(0, 2)
    turn(3)

    for s in range(seqs):
        rows = pl.ds(s, 1)
        par_buf[0, rows, :] = jnp.concatenate(
            [query_v[s, 0:1, :].astype(F32), query_v[s, 1:2, :].astype(F32)], axis=1
        )
        par_buf[1, rows, :] = jnp.concatenate(
            [key_v[s, 0:1, :].astype(F32), key_v[s, 1:2, :].astype(F32)], axis=1
        )
        par_buf[2, rows, :] = halves(nin_v[0:1, s : s + 1], nin_v[1:2, s : s + 1])
        par_buf[3, rows, :] = halves(nfg_v[0:1, s : s + 1], nfg_v[1:2, s : s + 1])
        fresh = value_v[s].astype(F32)
        spread = jnp.concatenate([fresh, jnp.zeros((2, 120), F32)], axis=1)
        left = pltpu.roll(spread, 8 * lax.rem(sp, 8), 1)
        fresh_row = halves(left[0:1], pltpu.roll(left[1:2], 64, 1))
        f_buf[s : s + 1, :] = jnp.where(sp < 8, fresh_row, 0.0)
        f_buf[4 + s : 5 + s, :] = jnp.where(sp < 8, 0.0, fresh_row)
    col_buf[:, 0:8] = jnp.transpose(
        jnp.concatenate(
            [taps_v[...].astype(F32), jnp.zeros((1, 128), F32), par_buf[0, 0:4, :]], axis=0
        )
    )

    bias_col = jnp.where(
        lax.broadcasted_iota(jnp.int32, (2, 1), 0) == 0, bias_v[0], bias_v[1]
    )

    cols_of = out_w.shape[2] // sp_n

    def ow_slot(ref):
        return ref.at[sp // 8, :, lax.rem(sp, 8)]

    def ow_cols(j):
        return out_w.at[:, :, pl.ds(pl.multiple_of(j * cols_of, cols_of), cols_of)]

    pos = lax.broadcasted_iota(jnp.int32, (1, length), 1)
    my_rows = pl.multiple_of(8 * sp, 8)
    my_tile = pl.multiple_of(8 * sp, 8)

    def slot_rows(s, size):
        return pl.ds(pl.multiple_of((s * sp_n + sp) * size, size), size)

    def rows_of(x):
        parts = [part.astype(F32) for part in three_parts(x)]
        return jnp.concatenate(parts + [jnp.zeros((10, length), F32)], axis=0).astype(BF16)

    def joined(x, h):
        return x[h : h + 1] + x[2 + h : 3 + h] + x[4 + h : 5 + h]

    def suffix(s):
        fg_pre = r_buf[s, 8:10, :].astype(BF16).astype(F32)
        log_f = log_sigmoid(fg_pre + bias_col) + extra_v[s]
        if s == seqs - 1:
            sums = jnp.dot(rows_of(log_f), tri_buf[...], preferred_element_type=F32)
            later = sums[0:2] + sums[2:4] + sums[4:6]
        else:
            later = jnp.where(pos < length - 1, pltpu.roll(log_f, length - 1, 1), 0.0)
            shift = 1
            while shift < length:
                later = later + jnp.where(
                    pos < length - shift, pltpu.roll(later, length - shift, 1), 0.0
                )
                shift *= 2
        suf_buf[s, 0:2, :] = later
        suf_buf[s, 2:4, :] = jnp.broadcast_to(later[:, 0:1] + log_f[:, 0:1], (2, length))

    def keys(s):
        key = r_buf[s, KEY0:VAL0, :].astype(BF16).astype(F32)
        edge = length - 128
        earlier = pltpu.roll(key, 1, 1)
        earlier = jnp.concatenate(
            [jnp.where(lane == 0, col_buf[:, 8 + s : 9 + s], earlier[:, :128]), earlier[:, 128:]],
            axis=1,
        )
        coming = pltpu.roll(key, length - 1, 1)
        coming = jnp.concatenate(
            [
                coming[:, :edge],
                jnp.where(lane == 127, col_buf[:, 16 + s : 17 + s], coming[:, edge:]),
            ],
            axis=1,
        )
        mixed = col_buf[:, 0:1] * earlier + col_buf[:, 1:2] * key + col_buf[:, 2:3] * coming
        key_rows = (mixed * jax.nn.sigmoid(mixed) * 0.125).astype(BF16)
        key_buf[s] = key_rows
        prod = key_rows.astype(F32) * col_buf[:, 4 + s : 5 + s]
        along = jnp.concatenate(
            [
                jnp.sum(prod[0:64], axis=0, keepdims=True),
                jnp.sum(prod[64:128], axis=0, keepdims=True),
            ],
            axis=0,
        )
        along_buf[s] = rows_of(along)

    def weigh(s):
        in_pre = r_buf[s, 0:2, :].astype(BF16).astype(F32)
        gate = in_pre + suf_buf[s, 0:2, :]
        top = jnp.max(gate, axis=1, keepdims=True)
        scale = jnp.exp(gate - top)
        lhs_buf[s, 0:16, :] = rows_of(scale)
        for h in range(2):
            value = r_buf[s, VAL0 + 128 * h : VAL0 + 128 * (h + 1), :].astype(BF16).astype(F32)
            lhs_buf[s, 16 + 128 * h : 144 + 128 * h, :] = (value * scale[h : h + 1]).astype(BF16)
        total = suf_buf[s, 2:4, 0:1]
        row = jnp.where(
            lax.rem(lane, 64) < 32,
            halves(total[0:1], total[1:2]),
            halves(top[0:1], top[1:2]),
        )
        e_buf[4 * s + 3 : 4 * s + 4, :] = row

    def outer(s):
        num_parts = lax.dot_general(
            along_buf[s], lhs_buf[s, 16:, :], NT, preferred_element_type=F32
        )
        both = lax.dot_general(lhs_buf[s], key_buf[s], NT, preferred_element_type=F32)
        num0 = joined(num_parts, 0)[:, 0:128]
        num1 = joined(num_parts, 1)[:, 128:256]
        e_buf[4 * s : 4 * s + 1, :] = halves(joined(both, 0), joined(both, 1))
        e_buf[4 * s + 1 : 4 * s + 2, :] = halves(num0, pltpu.roll(num1, 64, 1))
        e_buf[4 * s + 2 : 4 * s + 3, :] = halves(pltpu.roll(num0, 64, 1), num1)
        mem_buf[pl.ds(128 * s, 128), :] = halves(both[16:144], both[144:272])

    z, x = sp // 4, lax.rem(sp, 4)
    offsets = sorted(
        ((dz, dx) for dz in range(4) for dx in range(4) if dz or dx),
        key=lambda o: -(min(o[0], 4 - o[0]) + min(o[1], 4 - o[1])),
    )
    peers = [lax.rem(z + dz, 4) * 4 + lax.rem(x + dx, 4) for dz, dx in offsets]

    def send_sums(s):
        e_recv[slot_rows(s, 4), :] = e_buf[4 * s : 4 * s + 4, :]
        for j in peers:
            pltpu.make_async_remote_copy(
                src_ref=e_buf.at[pl.ds(4 * s, 4), :],
                dst_ref=e_recv.at[slot_rows(s, 4), :],
                send_sem=e_ssem,
                recv_sem=e_rsem.at[s // (seqs - 1)],
                device_id=(j, tp),
                device_id_type=MESH_ID,
            ).start()

    def send_memory(s):
        m_recv[slot_rows(s, 8), :] = mem_buf[pl.ds(128 * s + my_rows, 8), :]
        for j in peers:
            pltpu.make_async_remote_copy(
                src_ref=mem_buf.at[pl.ds(pl.multiple_of(128 * s + 8 * j, 8), 8), :],
                dst_ref=m_recv.at[slot_rows(s, 8), :],
                send_sem=m_ssem,
                recv_sem=m_rsem,
                device_id=(j, tp),
                device_id_type=MESH_ID,
            ).start()

    finished(p_copies[3:])
    landed(p_buf.at[1, :, pl.ds(0, width // 2)], p_sem.at[CHUNKS])
    start(s_copies[3], 1)
    chunk_dot(0, 3)
    chunk_dot(1, 0)
    chunk_dot(1, 1)
    suffix(0)
    landed(p_buf.at[1, :, pl.ds(width // 2, width // 2)], p_sem.at[CHUNKS + 1])
    chunk_dot(1, 2)
    chunk_dot(1, 3)

    landed(p_buf.at[2], p_sem.at[CHUNKS + 2])
    chunk_dot(2, 0)
    own_ow = pltpu.make_async_copy(ow_cols(sp), ow_slot(ow_recv), ow_local)
    own_ow.start()
    f_recv[pl.ds(my_tile, 8), :] = f_buf[...]
    for j in peers:
        pltpu.make_async_remote_copy(
            src_ref=f_buf,
            dst_ref=f_recv.at[pl.ds(my_tile, 8), :],
            send_sem=f_ssem,
            recv_sem=f_rsem,
            device_id=(j, tp),
            device_id_type=MESH_ID,
        ).start()
        pltpu.make_async_remote_copy(
            src_ref=ow_cols(j),
            dst_ref=ow_slot(ow_recv),
            send_sem=ow_ssem,
            recv_sem=ow_rsem,
            device_id=(j, tp),
            device_id_type=MESH_ID,
        ).start()

    chunk_dot(2, 1)
    suffix(1)
    landed(h_recv, h_rsem)
    col_buf[:, 8:16] = jnp.where(sp == 0, 0.0, jnp.transpose(h_recv[0]))
    col_buf[:, 16:24] = jnp.where(sp == sp_n - 1, 0.0, jnp.transpose(h_recv[1]))
    keys(0)
    weigh(0)
    chunk_dot(2, 2)
    chunk_dot(2, 3)

    landed(p_buf.at[3], p_sem.at[CHUNKS + 3])
    outer(0)
    chunk_dot(3, 0)
    keys(1)
    weigh(1)
    send_sums(0)
    send_memory(0)
    chunk_dot(3, 1)
    suffix(2)
    outer(1)
    chunk_dot(3, 2)
    keys(2)
    weigh(2)
    send_sums(1)
    chunk_dot(3, 3)
    outer(2)
    suffix(3)
    send_sums(2)
    keys(3)
    weigh(3)
    outer(3)
    send_sums(3)
    send_memory(1)
    send_memory(2)
    send_memory(3)

    def take(ref, sem, count):
        view = ref.at[pl.ds(0, count), :]
        pltpu.make_async_copy(view, view, sem).wait()

    own_ow.wait()
    ow_bytes = out_w.at[:, :, pl.ds(0, cols_of * (sp_n - 1))]
    pltpu.make_async_copy(ow_bytes, ow_bytes, ow_rsem).wait()
    ow_buf[...] = ow_recv[...].reshape(256, cols_of)
    take(f_recv, f_rsem, 8 * (sp_n - 1))
    fresh_sum = f_recv[0:8, :]
    for i in range(1, sp_n):
        fresh_sum = fresh_sum + f_recv[8 * i : 8 * i + 8, :]

    row16 = lax.broadcasted_iota(jnp.int32, (sp_n, 128), 0)
    low_lanes = lax.rem(lax.broadcasted_iota(jnp.int32, (sp_n, 128), 1), 64) < 32

    def by_head(x):
        left = jnp.sum(jnp.where(first_head, x, 0.0), axis=1, keepdims=True)
        right = jnp.sum(jnp.where(first_head, 0.0, x), axis=1, keepdims=True)
        return halves(left, right)

    def combine(s):
        def rows_at(k):
            return e_recv[pl.ds(s * sp_n * 4 + k, sp_n, stride=4), :]

        stats = rows_at(3)
        totals = jnp.where(low_lanes, stats, pltpu.roll(stats, 32, 1))
        tops = jnp.where(low_lanes, pltpu.roll(stats, 96, 1), stats)
        later = jnp.where(row16 < sp_n - 1, pltpu.roll(totals, sp_n - 1, 0), 0.0)
        shift = 1
        while shift < sp_n:
            later = later + jnp.where(
                row16 < sp_n - shift, pltpu.roll(later, sp_n - shift, 0), 0.0
            )
            shift *= 2
        gate = tops + later
        peak = jnp.max(gate, axis=0, keepdims=True)
        factor = jnp.exp(gate - peak)

        def summed(k):
            return jnp.sum(factor * rows_at(k), axis=0, keepdims=True)

        norm, num_a, num_b = summed(0), summed(1), summed(2)
        q, k = par_buf[0, s : s + 1, :], par_buf[1, s : s + 1, :]
        gate_in, gate_fg = par_buf[2, s : s + 1, :], par_buf[3, s : s + 1, :]
        kept = log_sigmoid(gate_fg) + peak
        new_peak = jnp.maximum(kept, gate_in)
        old_scale = jnp.exp(kept - new_peak)
        new_scale = jnp.exp(gate_in - new_peak)
        denom = jnp.maximum(jnp.abs(by_head(q * (old_scale * norm + new_scale * k))), 1.0)
        fresh_scale = new_scale * by_head(q * k)
        read_a = (old_scale * num_a + fresh_scale * fresh_sum[s : s + 1]) / denom
        read_b = (old_scale * num_b + fresh_scale * fresh_sum[4 + s : 5 + s]) / denom
        packed[32 + s : 33 + s, :] = pltpu.roll(norm, lax.rem(128 - 4 * sp, 128), 1)
        packed[36 + s : 37 + s, :] = peak
        return jnp.concatenate([read_a, read_b], axis=1), factor

    reads, factors = [], []
    take(e_recv, e_rsem.at[0], 4 * (sp_n - 1) * (seqs - 1))
    for s in range(seqs - 1):
        row, factor = combine(s)
        reads.append(row)
        factors.append(factor)
    take(e_recv, e_rsem.at[1], 4 * (sp_n - 1))
    row, factor = combine(seqs - 1)
    reads.append(row)
    factors.append(factor)

    read = jnp.concatenate(reads + [jnp.zeros((12, 256), F32)], axis=0).astype(BF16)
    part = jnp.dot(read, ow_buf[...], preferred_element_type=F32)[0:4]
    part_buf[0] = part[:, 0:128]
    part_buf[1] = part[:, 128:256]
    part_recv[tp] = part_buf[tp // 4]
    y, core = tp // 2, lax.rem(tp, 2)
    for dy, dc in ((2, 1), (2, 0), (1, 1), (3, 1), (1, 0), (3, 0), (0, 1)):
        j = lax.rem(y + dy, 4) * 2 + lax.rem(core + dc, 2)
        pltpu.make_async_remote_copy(
            src_ref=part_buf.at[j // 4],
            dst_ref=part_recv.at[tp],
            send_sem=o_ssem,
            recv_sem=o_rsem,
            device_id=(sp, j),
            device_id_type=MESH_ID,
        ).start()

    take(m_recv, m_rsem, 8 * (sp_n - 1) * seqs)
    for s in range(seqs):
        memory = jnp.zeros((8, 128), F32)
        for i in range(sp_n):
            base = (s * sp_n + i) * 8
            memory = memory + factors[s][i : i + 1] * m_recv[base : base + 8, :]
        packed[8 * s : 8 * s + 8, :] = memory

    view = part_recv.at[pl.ds(0, tp_n - 1)]
    pltpu.make_async_copy(view, view, o_rsem).wait()
    whole = part_recv[0]
    for i in range(1, tp_n):
        whole = whole + part_recv[i]
    packed[40:44, :] = pltpu.roll(whole, lax.rem(128 - 32 * lax.rem(tp, 4), 128), 1)

    landed(h_recv, h_ssem)
    pltpu.make_async_copy(ow_bytes, ow_bytes, ow_ssem).wait()
    take(f_recv, f_ssem, 8 * (sp_n - 1))
    take(e_recv, e_ssem, 4 * (sp_n - 1) * seqs)
    take(m_recv, m_ssem, 8 * (sp_n - 1) * seqs)
    pltpu.make_async_copy(view, view, o_ssem).wait()


def unpack(packed, mem_out, norm_out, peak_out, read_out):
    seqs = mem_out.shape[0]
    for s in range(seqs):
        rows = packed[8 * s : 8 * s + 8, :]
        mem_out[s, 0] = rows[:, 0:64].astype(BF16)
        mem_out[s, 1] = rows[:, 64:128].astype(BF16)
        norm = packed[32 + s : 33 + s, :]
        norm_out[s, 0:1, :] = norm[:, 0:4].astype(BF16)
        norm_out[s, 1:2, :] = norm[:, 64:68].astype(BF16)
        peak = packed[36 + s : 37 + s, :]
        peak_out[0:1, s : s + 1] = peak[:, 0:1]
        peak_out[1:2, s : s + 1] = peak[:, 64:65]
    read_out[...] = packed[40:44, 0:32].astype(BF16)


def body(
    prompt, key_weight, value_weight, input_gate_weight, forget_gate_weight, forget_bias,
    key_taps, extra_decay, new_query, new_key, new_value, new_input_gate, new_forget_gate,
    out_weight,
):
    seqs, length, width = prompt.shape
    sp_n = lax.axis_size("sp")
    tp_n = lax.axis_size("tp")
    cols_of = out_weight.shape[2] // sp_n
    any_spec = pl.BlockSpec(memory_space=pl.ANY)
    vmem = pl.BlockSpec(memory_space=pltpu.VMEM)
    dma = pltpu.SemaphoreType.DMA
    packed = pl.pallas_call(
        kernel,
        out_shape=pltpu.VMEM((48, 128), F32),
        in_specs=[any_spec] * 14,
        out_specs=vmem,
        scratch_shapes=[
            pltpu.VMEM((seqs, length, width), BF16),
            pltpu.VMEM((width, 128), BF16),
            pltpu.VMEM((width, 256), BF16),
            pltpu.VMEM((400, width), BF16),
            pltpu.VMEM((64, width), BF16),
            pltpu.VMEM((seqs, 400, length), F32),
            pltpu.VMEM((length, length), BF16),
            pltpu.VMEM((4, 8, 128), F32),
            pltpu.VMEM((seqs * 128, 128), F32),
            pltpu.VMEM((seqs * 4, 128), F32),
            pltpu.VMEM((2, 8, 128), F32),
            pltpu.VMEM((2, 8, 128), F32),
            pltpu.VMEM((seqs * sp_n * 4, 128), F32),
            pltpu.VMEM((seqs * sp_n * 8, 128), F32),
            pltpu.VMEM((2, 2, 8, 8, cols_of), BF16),
            pltpu.VMEM((2, 4, 128), F32),
            pltpu.VMEM((tp_n, 4, 128), F32),
            pltpu.VMEM((8, 128), F32),
            pltpu.VMEM((sp_n * 8, 128), F32),
            pltpu.VMEM((seqs, 272, length), BF16),
            pltpu.VMEM((seqs, 128, length), BF16),
            pltpu.VMEM((seqs, 16, length), BF16),
            pltpu.VMEM((seqs, 4, length), F32),
            pltpu.VMEM((256, cols_of), BF16),
            pltpu.VMEM((128, 128), F32),
            pltpu.VMEM((2, width), BF16),
            pltpu.VMEM((2, width), BF16),
            pltpu.SMEM((2,), F32),
            pltpu.VMEM((3, 128), BF16),
            pltpu.VMEM((seqs, 2, length), F32),
            pltpu.VMEM((seqs, 2, 64), BF16),
            pltpu.VMEM((seqs, 2, 64), BF16),
            pltpu.VMEM((seqs, 2, 8), BF16),
            pltpu.VMEM((2, seqs), F32),
            pltpu.VMEM((2, seqs), F32),
            dma((1 + CHUNKS,)),
            dma((CHUNKS + seqs,)),
            dma,
            dma((10,)),
            dma,
            dma,
            dma,
            dma,
            dma((2,)),
            dma,
            dma,
            dma,
            dma,
            dma,
            dma,
            dma,
            dma,
        ],
        compiler_params=pltpu.CompilerParams(
            collective_id=0, has_side_effects=True, vmem_limit_bytes=60 * 1024 * 1024
        ),
        name="prompt_state",
    )(
        prompt,
        key_weight,
        value_weight,
        input_gate_weight.T,
        forget_gate_weight.T,
        forget_bias,
        key_taps,
        jnp.transpose(extra_decay, (0, 2, 1)),
        new_query,
        new_key,
        new_value,
        new_input_gate.T,
        new_forget_gate.T,
        out_weight,
    )
    memory, norm, peak, read = pl.pallas_call(
        unpack,
        out_shape=(
            jax.ShapeDtypeStruct((seqs, 2, 8, 64), BF16),
            jax.ShapeDtypeStruct((seqs, 2, 4), BF16),
            jax.ShapeDtypeStruct((2, seqs), F32),
            jax.ShapeDtypeStruct((seqs, 32), BF16),
        ),
        in_specs=[vmem],
        out_specs=(vmem,) * 4,
        compiler_params=pltpu.CompilerParams(vmem_limit_bytes=1024 * 1024),
        name="unpack",
    )(packed)
    return jnp.transpose(memory, (0, 1, 3, 2)), norm, peak.T, read


def solution(mesh):
    in_specs = (
        P(None, "sp", None),
        P(None, "tp"),
        P(None, "tp"),
        P(None, "tp"),
        P(None, "tp"),
        P("tp"),
        P(None, "tp"),
        P(None, "sp", "tp"),
        P(None, "tp", None),
        P(None, "tp", None),
        P(None, "tp", "sp"),
        P(None, "tp"),
        P(None, "tp"),
        P("tp", "sp", None),
    )
    out_specs = (
        P(None, "tp", None, "sp"),
        P(None, "tp", "sp"),
        P(None, "tp"),
        P(None, ("sp", "tp")),
    )
    return jax.shard_map(body, mesh=mesh, in_specs=in_specs, out_specs=out_specs, check_vma=False)
```
